32 devices in a mesh: sp: 8 (over z, y), tp: 4 (over x, core).
Axes of the slice: x: 2, y: 2, z: 4, core: 2. Of those that a mesh axis runs over, the one named last changes fastest.
Arguments:
- out_grad: bfloat16 [1024, 2048], P('sp'), may hold values from -6 to 6
- residual: bfloat16 [1024, 2048], P('sp'), may hold values from -6 to 6
- routes: int32 [1024, 2], P('sp'), may hold values from 0 to 3, all different within a row; in each aligned block of 128 rows (0 to 127, 128 to 255, ...) at most 80 rows name the same one
- route_weights: float32 [1024, 2], P('sp'), may hold values from 0.15 to 0.85, as said below
- w_gate: bfloat16 [8, 2048, 2048], P('sp', None, 'tp'), may hold values from -0.125 to 0.125
- w_up: bfloat16 [8, 2048, 2048], P('sp', None, 'tp'), may hold values from -0.125 to 0.125
- w_down: bfloat16 [8, 2048, 2048], P('sp', 'tp'), may hold values from -0.09375 to 0.09375
- out_gate: bfloat16 [1024, 1024], P('sp', 'tp'), may hold values from -6 to 6
- in_gate: bfloat16 [1024, 1024], P('sp', 'tp'), may hold values from -6 to 6
- conv_input: bfloat16 [1024, 1024], P('sp', 'tp'), may hold values from -6 to 6
- conv_out: bfloat16 [1024, 1024], P('sp', 'tp'), may hold values from -6 to 6
- conv_taps: float32 [3, 1024], P(None, 'tp'), may hold values from -3.5 to 3.5
- w_out: bfloat16 [1024, 2048], P('tp'), may hold values from -0.1875 to 0.1875
Outputs:
- grad_resid: bfloat16 [1024, 2048], P('sp')
- grad_up: bfloat16 [8, 2048, 2048], P('sp', None, 'tp')
- grad_down: bfloat16 [8, 2048, 2048], P('sp', 'tp')
- grad_out_gate: bfloat16 [1024, 1024], P('sp', 'tp')
- grad_in_gate: bfloat16 [1024, 1024], P('sp', 'tp')
- grad_conv_input: bfloat16 [1024, 1024], P('sp', 'tp')
- grad_w_out: float32 [2048, 1024], P('sp', 'tp')
The draws below stay inside these ranges and needn't reach their ends.
Inputs may be any that keep to these rules, and one draw needn't show every extreme that they name: `routes`: each row names 2 different experts. In the rows of one index of sp no expert is named more than 80 times, a bound that some block reaches. `route_weights`: the two weights of a row sum to one.
All inputs are finite; a program needn't handle non-finite values.
Results may differ from the reference program's by a relative error of at most 0.013.
Values may be sent and summed in bfloat16 or wider, within the bound.
No kernel may reach another device: no remote copies, remote signals or barrier semaphores. Data moves between devices by JAX's collectives and lax.ppermute only.
A program may use at most 128 MiB of HBM per device.

```python
import math
import jax
import jax.numpy as jnp
import numpy as np
from jax import lax

D = 2048
FF_HALF = 2048
SC = 1024
TOP_K = 2
TOK_DEV = 128
TOKENS = 1024
EXPERTS = 4
SLICES = 8
CAP = 80
N_SP = 8
N_TP = 4


def draw_route_weights(key, part):
    leading = jax.random.uniform(key, (TOKENS, 1), jnp.float32, 0.15, 0.85)
    return jnp.concatenate([leading, 1.0 - leading], axis=1)


def with_spikes(array, key, source, target, shards_of, factor):
    owner, partner = [(jnp.arange(array.shape[dim]) // (array.shape[dim] // shards_of)).reshape([-1 if axis == dim else 1 for axis in range(array.ndim)]) for dim in (source, target)]
    chosen = jax.random.permutation(key, shards_of)[partner]
    strong = (owner == chosen) | (owner == (partner + shards_of // 2) % shards_of)
    return jnp.where(strong, factor * array, array)


def steps_of(rng, dims, pieces, least, largest):
    factor_of, own = 1.0, jax.random.fold_in(rng, 6)
    for position, parts in pieces:
        draws = jnp.exp(jax.random.uniform(jax.random.fold_in(own, position), (parts,), jnp.float32, least / len(pieces), largest / len(pieces)))
        factor_of = factor_of * jnp.repeat(draws, dims[position] // parts).reshape([-1 if axis == position else 1 for axis in range(len(dims))])
    return factor_of


def shared_out(own_key, own, number, rows, count, top, reach, lean):
    order = jax.random.permutation(own_key, count)
    heavy_load, usual = load_shares(count, rows * top, reach, lean, True), load_shares(count, rows * top, reach, lean, False)
    places = jnp.arange(count)

    def named(tallies, rotation):
        used = int((tallies > 0).sum())
        fixed = max(1, used // 4)
        passed = fixed + (places - fixed + rotation * (used - fixed)) % max(1, count - fixed)
        return jnp.zeros((count,), jnp.int32).at[order[jnp.where(places < fixed, places, passed)]].set(jnp.asarray(tallies, jnp.int32))

    tallies = jnp.where(number % 4 == 0, named(heavy_load, number // 4), named(usual, number - number // 4 - 1))
    mixed = jax.random.permutation(jax.random.fold_in(own, 3), count)
    source_of, receiver = mixed[0:count // 2 * 2:2], mixed[1:count // 2 * 2:2]
    slack = jnp.minimum(tallies[source_of] - 1, reach - tallies[receiver]) // 2
    slack = jnp.where((source_of == order[0]) | (receiver == order[0]) | (tallies[receiver] == 0), 0, jnp.maximum(slack, 0))
    passed = jax.random.randint(jax.random.fold_in(own, 4), (count // 2,), 0, 1 << 20) % (slack + 1)
    tallies = tallies.at[source_of].add(-passed).at[receiver].add(passed)
    members = jnp.searchsorted(jnp.cumsum(tallies), jnp.arange(rows * top), side="right").astype(jnp.int32)
    grid = members.reshape(top, rows).T
    grid = grid[jax.random.permutation(jax.random.fold_in(own, 1), rows)]
    rotation = jax.random.randint(jax.random.fold_in(own, 2), (rows, 1), 0, top)
    return jnp.take_along_axis(grid, (jnp.arange(top)[None, :] + rotation) % top, axis=1)


def load_shares(amount, total, reach, slope, full):
    portions = [(1 << 20) // math.isqrt(grade ** slope) + 1 for grade in range(1, amount + 1)]
    largest = reach if full else min(reach, max(-(-total // amount), total * portions[0] // sum(portions)))
    least = 1 if total - largest >= amount - 1 else 0
    counts, surplus = [largest] + [least] * (amount - 1), total - largest - least * (amount - 1)
    while surplus > 0:
        candidates = [i for i in range(1, amount) if counts[i] < largest] or [i for i in range(1, amount) if counts[i] < reach]
        whole, remaining = sum([portions[i] for i in candidates]), surplus
        for i in candidates:
            addition = min(reach - counts[i], max(1, remaining * portions[i] // whole), surplus)
            counts[i] = counts[i] + addition
            surplus = surplus - addition
    return np.array(counts)


def scatter_about(key, shape, scale, limit, pieces=(), held_as=jnp.bfloat16):
    entries = scale * jax.random.normal(key, shape, jnp.float32)
    if pieces:
        entries = entries * steps_of(key, shape, pieces, -0.22, 0.18)
    return jnp.clip(entries, -limit, limit).astype(held_as)


def noise_with(stream_key, dims, spread, reach, shards, heavy, kind=jnp.bfloat16):
    entries = spread * jax.random.normal(stream_key, dims, jnp.float32)
    if shards:
        entries = entries * steps_of(stream_key, dims, shards, -0.22, 0.18)
    return jnp.clip(with_spikes(entries, jax.random.fold_in(stream_key, 3), *heavy), -reach, reach).astype(kind)


def setup_inputs(seed: int = 0) -> dict:
    keys = jax.random.split(jax.random.key(seed), 14)
    out_grad = noise_with(keys[0], (TOKENS, D), 1.0, 6.0, ((0, 8),), (0, 1, 8, 2.0))
    residual = scatter_about(keys[1], (TOKENS, D), 1.0, 6.0, ((0, 8),))
    routes_keys = jax.random.split(jax.random.fold_in(keys[2], 1), TOKENS // TOK_DEV)
    routes_turns = jax.random.permutation(jax.random.fold_in(keys[2], 3), TOKENS // TOK_DEV)
    routes = jax.vmap(lambda own, number: shared_out(jax.random.fold_in(keys[2], 2), own, number, TOK_DEV, EXPERTS, TOP_K, CAP, 1))(routes_keys, routes_turns).reshape((TOKENS, TOP_K))
    route_weights = draw_route_weights(jax.random.fold_in(keys[13], 71), 0)
    w_gate = scatter_about(keys[4], (SLICES, D, FF_HALF), D ** -0.5, 0.125, ((0, 8), (2, 4)))
    w_up = scatter_about(keys[5], (SLICES, D, FF_HALF), D ** -0.5, 0.125, ((0, 8), (2, 4)))
    w_down = scatter_about(keys[6], (SLICES, FF_HALF, D), (2 * FF_HALF) ** -0.5, 0.09375, ((0, 8), (1, 4)))
    out_gate = scatter_about(keys[7], (TOKENS, SC), 1.0, 6.0, ((0, 8), (1, 4)))
    in_gate = scatter_about(keys[8], (TOKENS, SC), 1.0, 6.0, ((0, 8), (1, 4)))
    conv_input = scatter_about(keys[9], (TOKENS, SC), 1.0, 6.0, ((0, 8), (1, 4)))
    conv_out = scatter_about(keys[10], (TOKENS, SC), 1.0, 6.0, ((0, 8), (1, 4)))
    conv_taps = scatter_about(keys[11], (3, SC), 3 ** -0.5, 3.5, ((1, 4),), jnp.float32)
    w_out = scatter_about(keys[12], (SC, D), SC ** -0.5, 0.1875, ((0, 4),))
    return dict(out_grad=out_grad, residual=residual, routes=routes, route_weights=route_weights, w_gate=w_gate, w_up=w_up, w_down=w_down, out_gate=out_gate, in_gate=in_gate, conv_input=conv_input, conv_out=conv_out, conv_taps=conv_taps, w_out=w_out)


epsilon = 1e-06

def reference(out_grad, residual, routes, route_weights, w_gate, w_up, w_down, out_gate, in_gate, conv_input, conv_out, conv_taps, w_out):
    resid_f32 = residual.astype(jnp.float32)
    inv_rms = lax.rsqrt(lax.optimization_barrier(jnp.mean(resid_f32 * resid_f32, axis=-1, keepdims=True)) + epsilon)
    unit_rows = resid_f32 * inv_rms
    normed = unit_rows.astype(jnp.bfloat16)
    n_assign = TOKENS * TOP_K
    weighted = (route_weights[:, :, None] * out_grad.astype(jnp.float32)[:, None, :]).astype(jnp.bfloat16).reshape(n_assign, D)
    flat_routes = routes.reshape(-1).astype(jnp.int32)
    onehot = (flat_routes[:, None] == jnp.arange(EXPERTS, dtype=jnp.int32)[None, :]).astype(jnp.int32)
    blocks = onehot.reshape(N_SP, TOP_K * TOK_DEV, EXPERTS)
    before = (jnp.cumsum(blocks, axis=1) - blocks).reshape(n_assign, EXPERTS)
    slot_rank = lax.optimization_barrier(jnp.sum(before * onehot, axis=1)).astype(jnp.int32)
    source = (jnp.arange(n_assign, dtype=jnp.int32) // (TOP_K * TOK_DEV)).astype(jnp.int32)
    slot_table = jnp.full((EXPERTS, N_SP * CAP), n_assign, jnp.int32)
    slot_table = slot_table.at[flat_routes, source * CAP + slot_rank].set(jnp.arange(n_assign, dtype=jnp.int32))
    quarter = FF_HALF // N_TP
    n_blocks = 2 * N_TP

    def one_expert(expert):
        slot_ids = slot_table[expert]
        filled = slot_ids < n_assign
        safe_ids = jnp.where(filled, slot_ids, 0)
        expert_rows = jnp.where(filled[:, None], normed[safe_ids // TOP_K], jnp.zeros((), jnp.bfloat16))
        expert_grads = jnp.where(filled[:, None], weighted[safe_ids], jnp.zeros((), jnp.bfloat16))
        gate_full = jnp.concatenate([w_gate[2 * expert], w_gate[2 * expert + 1]], axis=1)
        up_full = jnp.concatenate([w_up[2 * expert], w_up[2 * expert + 1]], axis=1)
        down_full = jnp.concatenate([w_down[2 * expert], w_down[2 * expert + 1]], axis=0)
        pre_gate = jnp.dot(expert_rows, gate_full, preferred_element_type=jnp.float32)
        pre_up = jnp.dot(expert_rows, up_full, preferred_element_type=jnp.float32)
        sigmoid_gate = jax.nn.sigmoid(pre_gate)
        activated = pre_gate * sigmoid_gate
        hidden = (activated * pre_up).astype(jnp.bfloat16)
        d_hidden = jnp.dot(expert_grads, down_full.T, preferred_element_type=jnp.float32)
        grad_down = jnp.dot(hidden.T, expert_grads, preferred_element_type=jnp.float32).astype(jnp.bfloat16)
        d_gate = (d_hidden * pre_up * sigmoid_gate * (1.0 + pre_gate * (1.0 - sigmoid_gate))).astype(jnp.bfloat16)
        d_up = (d_hidden * activated).astype(jnp.bfloat16)
        grad_up = jnp.dot(expert_rows.T, d_up, preferred_element_type=jnp.float32).astype(jnp.bfloat16)
        partial_value = jnp.einsum('rjf,djf->jrd', d_gate.astype(jnp.float32).reshape(-1, n_blocks, quarter), gate_full.astype(jnp.float32).reshape(D, n_blocks, quarter))
        partial_value = partial_value + jnp.einsum('rjf,djf->jrd', d_up.astype(jnp.float32).reshape(-1, n_blocks, quarter), up_full.astype(jnp.float32).reshape(D, n_blocks, quarter))
        partial_value = lax.optimization_barrier(partial_value.astype(jnp.bfloat16)).astype(jnp.float32)
        slice_sum = lax.optimization_barrier(jnp.sum(partial_value.reshape(2, N_TP, -1, D), axis=1)).astype(jnp.bfloat16)
        down_pair = grad_down.reshape(2, FF_HALF, D)
        up_pair = jnp.transpose(grad_up.reshape(D, 2, FF_HALF), (1, 0, 2))
        return (down_pair, up_pair, slice_sum, slot_ids)
    down_all, up_all, sums_all, ids_all = lax.map(one_expert, jnp.arange(EXPERTS, dtype=jnp.int32))
    grad_down = down_all.reshape(SLICES, FF_HALF, D)
    grad_up = up_all.reshape(SLICES, D, FF_HALF)
    contrib = lax.optimization_barrier(jnp.sum(sums_all.astype(jnp.float32), axis=1)).reshape(-1, D)
    collected = jnp.zeros((n_assign + 1, D), jnp.float32).at[ids_all.reshape(-1)].add(contrib)
    d_normed = lax.optimization_barrier(jnp.sum(collected[:n_assign].reshape(TOKENS, TOP_K, D), axis=1))
    row_mean = lax.optimization_barrier(jnp.mean(unit_rows * d_normed, axis=-1, keepdims=True))
    grad_resid = (out_grad.astype(jnp.float32) + inv_rms * (d_normed - unit_rows * row_mean)).astype(jnp.bfloat16)
    d_mix = jnp.dot(grad_resid, w_out.T, preferred_element_type=jnp.float32)
    conv_f32 = conv_out.astype(jnp.float32)
    gate_f32 = out_gate.astype(jnp.float32)
    grad_out_gate = (d_mix * conv_f32).astype(jnp.bfloat16)
    d_conv = d_mix * gate_f32
    padded = jnp.pad(d_conv, ((1, 1), (0, 0)))
    taps_f32 = conv_taps.astype(jnp.float32)
    d_inner = taps_f32[0] * padded[2:] + taps_f32[1] * padded[1:-1] + taps_f32[2] * padded[:-2]
    grad_in_gate = (d_inner * conv_input.astype(jnp.float32)).astype(jnp.bfloat16)
    grad_conv_input = (d_inner * in_gate.astype(jnp.float32)).astype(jnp.bfloat16)
    mixed = (gate_f32 * conv_f32).astype(jnp.bfloat16)
    grad_w_out = jnp.dot(grad_resid.T, mixed, preferred_element_type=jnp.float32)
    return (grad_resid, grad_up, grad_down, grad_out_gate, grad_in_gate, grad_conv_input, grad_w_out)
```

```python
import functools

import jax
import jax.numpy as jnp
from jax import lax
from jax.experimental import pallas as pl
from jax.experimental.pallas import tpu as pltpu
from jax.sharding import Mesh
from jax.sharding import PartitionSpec as P

epsilon = 1e-06
F32 = jnp.float32
BF16 = jnp.bfloat16


def swap(value, axis):
    return lax.ppermute(value, axis, [(0, 1), (1, 0)])


def swap_both(value):
    return lax.ppermute(value, ("j", "x"), [(i, 3 - i) for i in range(4)])


def shifted(value, step):
    count = lax.axis_size("e")
    return lax.ppermute(value, "e", [(i, (i + step) % count) for i in range(count)])


def dot(a, b, ca, cb):
    return lax.dot_general(a, b, (((ca,), (cb,)), ((), ())), preferred_element_type=F32)


def prepare(experts, cap, quarter, index_ref, routes_ref, weights_ref, resid_ref, grad_ref, *outs):
    sends, sel_ref = outs[:-1], outs[-1]
    tokens = resid_ref.shape[0]
    mine, column = index_ref[0], index_ref[1]
    resid = resid_ref[...].astype(F32)
    inv_rms = lax.rsqrt(jnp.mean(resid * resid, axis=-1, keepdims=True) + epsilon)
    cols = pl.ds(pl.multiple_of(column * quarter, quarter), quarter)
    normed = (resid_ref[:, cols].astype(F32) * inv_rms).astype(BF16)
    grad = grad_ref[:, cols]
    first, second = routes_ref[0:1, :], routes_ref[1:2, :]
    first = jnp.where(first >= mine, first - mine, first - mine + experts)
    second = jnp.where(second >= mine, second - mine, second - mine + experts)
    ids = lax.broadcasted_iota(jnp.int32, (experts, tokens), 0)
    in_first, in_second = ids == first, ids == second
    member = jnp.where(in_first | in_second, 1.0, 0.0)
    before = jnp.where(
        lax.broadcasted_iota(jnp.int32, (tokens, tokens), 0)
        < lax.broadcasted_iota(jnp.int32, (tokens, tokens), 1),
        1.0,
        0.0,
    )
    rank = dot(member.astype(BF16), before.astype(BF16), 1, 0)
    rank_first = jnp.sum(jnp.where(in_first, rank, 0.0), axis=0, keepdims=True).astype(jnp.int32)
    rank_second = jnp.sum(jnp.where(in_second, rank, 0.0), axis=0, keepdims=True).astype(jnp.int32)
    slot_first = first * cap + rank_first
    slot_second = second * cap + rank_second
    for step in range(experts):
        slots = lax.broadcasted_iota(jnp.int32, (cap, tokens), 0) + step * cap
        hit_first, hit_second = slots == slot_first, slots == slot_second
        pick = jnp.where(hit_first | hit_second, 1.0, 0.0).astype(BF16)
        share = jnp.where(hit_first, weights_ref[0:1, :], 0.0) + jnp.where(
            hit_second, weights_ref[1:2, :], 0.0
        )
        share = jnp.sum(share, axis=1, keepdims=True)
        sel_ref[step] = pick
        sends[step][0] = dot(pick, normed, 1, 0).astype(BF16)
        sends[step][1] = (share * dot(pick, grad, 1, 0)).astype(BF16)


def relative(value, axis, place):
    width = value.shape[axis] // 4
    parts = []
    for dc in range(2):
        for dx in range(2):
            parts.append(
                lax.dynamic_slice_in_dim(value, (place ^ (2 * dx + dc)) * width, width, axis)
            )
    return parts


def absolute(value, axis, place):
    width = value.shape[axis] // 4
    parts = []
    for q in range(4):
        r = place ^ q
        parts.append(
            lax.dynamic_slice_in_dim(value, ((r & 1) * 2 + (r >> 1)) * width, width, axis)
        )
    return jnp.concatenate(parts, axis=axis)


def per_device(
    out_grad,
    residual,
    routes,
    route_weights,
    w_gate,
    w_up,
    w_down,
    out_gate,
    in_gate,
    conv_input,
    conv_out,
    conv_taps,
    w_out,
):
    tokens, features = out_grad.shape
    experts = lax.axis_size("e")
    slices = 2 * experts
    cap = 5 * tokens // slices
    quarter = features // 4
    mine, half, core = lax.axis_index("e"), lax.axis_index("j"), lax.axis_index("c")
    place = 2 * lax.axis_index("x") + core

    outs = pl.pallas_call(
        functools.partial(prepare, experts, cap, quarter),
        out_shape=[jax.ShapeDtypeStruct((2, cap, quarter), BF16)] * experts
        + [jax.ShapeDtypeStruct((experts, cap, tokens), BF16)],
        in_specs=[pl.BlockSpec(memory_space=pltpu.SMEM)]
        + [pl.BlockSpec(memory_space=pltpu.VMEM)] * 4,
        out_specs=[pl.BlockSpec(memory_space=pltpu.VMEM)] * (experts + 1),
    )(
        jnp.stack([mine, place]).astype(jnp.int32),
        routes.T,
        route_weights.T,
        residual,
        out_grad,
    )
    sends, sel = outs[:-1], outs[-1]
    came = [sends[0]] + [shifted(sends[s], s) for s in range(1, experts)]
    rows_z = jnp.concatenate([b[0] for b in came], axis=0)
    grads_z = jnp.concatenate([b[1] for b in came], axis=0)
    count = rows_z.shape[0]

    rows_x, grads_y = swap(rows_z, "x"), swap(grads_z, "j")
    rows_pair = jnp.stack([rows_z, rows_x])
    grads_pair = jnp.stack([grads_z, grads_y])
    rows_four = jnp.stack([rows_pair, swap(rows_pair, "j")])
    grads_four = jnp.stack([grads_pair, swap(grads_pair, "x")])
    rows_sib, grads_sib = swap(rows_four, "c"), swap(grads_four, "c")
    rows = jnp.concatenate(
        [rows_four[:, 0], rows_four[:, 1], rows_sib[:, 0], rows_sib[:, 1]], axis=-1
    ).reshape(2 * count, features)
    grads = jnp.concatenate(
        [grads_four[0], grads_four[1], grads_sib[0], grads_sib[1]], axis=-1
    ).reshape(2 * count, features)

    gate_w = jnp.concatenate(relative(w_gate[0], 0, place), axis=0)
    up_w = jnp.concatenate(relative(w_up[0], 0, place), axis=0)
    down_w = jnp.concatenate(relative(w_down[0], 1, place), axis=1)
    pre_gate = dot(rows, gate_w, 1, 0)
    pre_up = dot(rows, up_w, 1, 0)
    sigmoid_gate = jax.nn.sigmoid(pre_gate)
    activated = pre_gate * sigmoid_gate
    hidden = (activated * pre_up).astype(BF16)
    d_hidden = dot(grads, down_w, 1, 1)
    d_gate = (d_hidden * pre_up * sigmoid_gate * (1.0 + pre_gate * (1.0 - sigmoid_gate))).astype(
        BF16
    )
    d_up = (d_hidden * activated).astype(BF16)

    split = features // 2
    away = dot(d_gate, gate_w[split:], 1, 1) + dot(d_up, up_w[split:], 1, 1)
    other = swap(away.astype(BF16), "c")
    kept = dot(d_gate, gate_w[:split], 1, 1) + dot(d_up, up_w[:split], 1, 1)
    total = (kept + other.astype(F32)).astype(BF16)
    block = lambda dj, dx: total[dj * count : (dj + 1) * count, dx * quarter : (dx + 1) * quarter]
    summed = (
        block(0, 0).astype(F32)
        + swap(block(0, 1), "x").astype(F32)
        + swap(block(1, 0), "j").astype(F32)
        + swap_both(block(1, 1)).astype(F32)
    ).astype(BF16)
    back = [summed[:cap]] + [
        shifted(summed[s * cap : (s + 1) * cap], -s) for s in range(1, experts)
    ]

    grad_up = absolute(dot(rows, d_up, 0, 0).astype(BF16), 0, place)
    grad_down = absolute(dot(hidden, grads, 0, 0).astype(BF16), 1, place)

    d_part = dot(
        sel.reshape(experts * cap, tokens), jnp.concatenate(back, axis=0), 0, 0
    ).astype(BF16)
    d_normed = lax.all_gather(d_part, ("x", "c"), axis=1, tiled=True).astype(F32)
    resid_f32 = residual.astype(F32)
    inv_rms = lax.rsqrt(jnp.mean(resid_f32 * resid_f32, axis=-1, keepdims=True) + epsilon)
    unit_rows = resid_f32 * inv_rms
    row_mean = jnp.mean(unit_rows * d_normed, axis=-1, keepdims=True)
    grad_resid = (out_grad.astype(F32) + inv_rms * (d_normed - unit_rows * row_mean)).astype(BF16)

    conv_f32 = conv_out.astype(F32)
    gate_f32 = out_gate.astype(F32)
    mixed = (gate_f32 * conv_f32).astype(BF16)
    mixed_pair = jnp.stack([mixed, swap(mixed, "j")])
    mixed_rel = jnp.stack([mixed_pair] + [shifted(mixed_pair, s) for s in range(1, experts)])
    channels = mixed.shape[1]
    mixed_rel = mixed_rel.reshape(slices, tokens, channels)
    mixed_all = jnp.concatenate(
        [
            lax.dynamic_slice_in_dim(
                mixed_rel, lax.rem(mine - e + experts, experts) * 2 + (half ^ j), 1, 0
            )
            for e in range(experts)
            for j in range(2)
        ],
        axis=0,
    )
    part = tokens // 2
    ordered = [
        lax.dynamic_slice_in_dim(mixed_all, (core ^ d) * part, part, 1).reshape(-1, channels)
        for d in range(2)
    ]
    width = features // slices
    mine_rows = lax.dynamic_slice_in_dim(grad_resid, core * part, part, 0)
    blocks = jnp.transpose(mine_rows.reshape(part, slices, width), (1, 0, 2))
    got = lax.all_to_all(blocks, ("e", "j"), 0, 0, tiled=True).reshape(slices * part, width)
    got_sib = swap(got, "c")
    grad_w_out = dot(got, ordered[0], 0, 0) + dot(got_sib, ordered[1], 0, 0)

    d_mix = dot(grad_resid, w_out, 1, 1)
    grad_out_gate = (d_mix * conv_f32).astype(BF16)
    d_conv = d_mix * gate_f32
    edge = d_conv.astype(BF16)
    ends = slices - 1
    above = lax.ppermute(edge[-1:], ("e", "j"), [(i, i + 1) for i in range(ends)]).astype(F32)
    below = lax.ppermute(edge[:1], ("e", "j"), [(i + 1, i) for i in range(ends)]).astype(F32)
    later = jnp.concatenate([d_conv[1:], below], axis=0)
    earlier = jnp.concatenate([above, d_conv[:-1]], axis=0)
    d_inner = conv_taps[0] * later + conv_taps[1] * d_conv + conv_taps[2] * earlier
    grad_in_gate = (d_inner * conv_input.astype(F32)).astype(BF16)
    grad_conv_input = (d_inner * in_gate.astype(F32)).astype(BF16)
    return (
        grad_resid,
        grad_up[None],
        grad_down[None],
        grad_out_gate,
        grad_in_gate,
        grad_conv_input,
        grad_w_out,
    )


def solution(mesh):
    slices, blocks = mesh.shape["sp"], mesh.shape["tp"]
    grid = mesh.devices.reshape(slices // 2, 2, blocks // 2, 2)
    inner = Mesh(grid, ("e", "j", "x", "c"))
    sp, tp = ("e", "j"), ("x", "c")
    in_specs = (
        P(sp, None),
        P(sp, None),
        P(sp, None),
        P(sp, None),
        P(sp, None, tp),
        P(sp, None, tp),
        P(sp, tp, None),
        P(sp, tp),
        P(sp, tp),
        P(sp, tp),
        P(sp, tp),
        P(None, tp),
        P(tp, None),
    )
    out_specs = (
        P(sp, None),
        P(sp, None, tp),
        P(sp, tp, None),
        P(sp, tp),
        P(sp, tp),
        P(sp, tp),
        P(sp, tp),
    )
    return jax.shard_map(
        per_device, mesh=inner, in_specs=in_specs, out_specs=out_specs, check_vma=False
    )
```

```python
import functools

import jax
import jax.numpy as jnp
from jax import lax
from jax.experimental import pallas as pl
from jax.experimental.pallas import tpu as pltpu
from jax.sharding import Mesh
from jax.sharding import PartitionSpec as P


epsilon = 1e-06
F32 = jnp.float32
BF16 = jnp.bfloat16


def swap(value, axis):
    return lax.ppermute(value, axis, [(0, 1), (1, 0)])


def swap_both(value):
    return lax.ppermute(value, ("j", "x"), [(i, 3 - i) for i in range(4)])


def exchange(blocks, sign):
    count = lax.axis_size("e")
    if count <= 8:
        return [
            lax.ppermute(b, "e", [(i, (i + sign * s) % count) for i in range(count)])
            for s, b in enumerate(blocks)
            if s
        ]
    mine, order = lax.axis_index("e"), jnp.arange(count)
    to = jnp.take(jnp.stack(blocks), sign * (order - mine) % count, axis=0)
    came = lax.all_to_all(to, "e", 0, 0, tiled=True)
    came = jnp.take(came, (mine - sign * order) % count, axis=0)
    return [came[s] for s in range(1, count)]


def dot(a, b, ca, cb):
    return lax.dot_general(a, b, (((ca,), (cb,)), ((), ())), preferred_element_type=F32)


def prepare(experts, cap, quarter, index_ref, routes_ref, weights_ref, resid_ref, grad_ref, *outs):
    sends, sel_ref = outs[:-1], outs[-1]
    tokens = resid_ref.shape[0]
    mine, column = index_ref[0], index_ref[1]
    resid = resid_ref[...].astype(F32)
    inv_rms = lax.rsqrt(jnp.mean(resid * resid, axis=-1, keepdims=True) + epsilon)
    cols = pl.ds(pl.multiple_of(column * quarter, quarter), quarter)
    normed = (resid_ref[:, cols].astype(F32) * inv_rms).astype(BF16)
    grad = grad_ref[:, cols]
    first, second = routes_ref[0:1, :], routes_ref[1:2, :]
    first = jnp.where(first >= mine, first - mine, first - mine + experts)
    second = jnp.where(second >= mine, second - mine, second - mine + experts)
    ids = lax.broadcasted_iota(jnp.int32, (experts, tokens), 0)
    in_first, in_second = ids == first, ids == second
    member = jnp.where(in_first | in_second, 1.0, 0.0)
    before = jnp.where(
        lax.broadcasted_iota(jnp.int32, (tokens, tokens), 0)
        < lax.broadcasted_iota(jnp.int32, (tokens, tokens), 1),
        1.0,
        0.0,
    )
    rank = dot(member.astype(BF16), before.astype(BF16), 1, 0)
    rank_first = jnp.sum(jnp.where(in_first, rank, 0.0), axis=0, keepdims=True).astype(jnp.int32)
    rank_second = jnp.sum(jnp.where(in_second, rank, 0.0), axis=0, keepdims=True).astype(jnp.int32)
    slot_first = first * cap + rank_first
    slot_second = second * cap + rank_second
    for step in range(experts):
        slots = lax.broadcasted_iota(jnp.int32, (cap, tokens), 0) + step * cap
        hit_first, hit_second = slots == slot_first, slots == slot_second
        pick = jnp.where(hit_first | hit_second, 1.0, 0.0).astype(BF16)
        share = jnp.where(hit_first, weights_ref[0:1, :], 0.0) + jnp.where(
            hit_second, weights_ref[1:2, :], 0.0
        )
        share = jnp.sum(share, axis=1, keepdims=True)
        sel_ref[step] = pick
        sends[step][0] = dot(pick, normed, 1, 0).astype(BF16)
        sends[step][1] = (share * dot(pick, grad, 1, 0)).astype(BF16)


def relative(value, axis, place):
    width = value.shape[axis] // 4
    parts = []
    for dc in range(2):
        for dx in range(2):
            parts.append(
                lax.dynamic_slice_in_dim(value, (place ^ (2 * dx + dc)) * width, width, axis)
            )
    return parts


def absolute(value, axis, place):
    width = value.shape[axis] // 4
    parts = []
    for q in range(4):
        r = place ^ q
        parts.append(
            lax.dynamic_slice_in_dim(value, ((r & 1) * 2 + (r >> 1)) * width, width, axis)
        )
    return jnp.concatenate(parts, axis=axis)


def per_device(
    out_grad,
    residual,
    routes,
    route_weights,
    w_gate,
    w_up,
    w_down,
    out_gate,
    in_gate,
    conv_input,
    conv_out,
    conv_taps,
    w_out,
):
    tokens, features = out_grad.shape
    experts = lax.axis_size("e")
    slices = 2 * experts
    cap = 5 * tokens // slices
    quarter = features // 4
    mine, half, core = lax.axis_index("e"), lax.axis_index("j"), lax.axis_index("c")
    place = 2 * lax.axis_index("x") + core

    outs = pl.pallas_call(
        functools.partial(prepare, experts, cap, quarter),
        out_shape=[jax.ShapeDtypeStruct((2, cap, quarter), BF16)] * experts
        + [jax.ShapeDtypeStruct((experts, cap, tokens), BF16)],
        in_specs=[pl.BlockSpec(memory_space=pltpu.SMEM)]
        + [pl.BlockSpec(memory_space=pltpu.VMEM)] * 4,
        out_specs=[pl.BlockSpec(memory_space=pltpu.VMEM)] * (experts + 1),
    )(
        jnp.stack([mine, place]).astype(jnp.int32),
        routes.T,
        route_weights.T,
        residual,
        out_grad,
    )
    sends, sel = outs[:-1], outs[-1]
    conv_f32 = conv_out.astype(F32)
    gate_f32 = out_gate.astype(F32)
    mixed = (gate_f32 * conv_f32).astype(BF16)
    mixed_pair = jnp.stack([mixed, swap(mixed, "j")])

    came = exchange(sends, 1)
    own_pair = jnp.stack([sends[0], swap(sends[0], "x")])
    own_four = jnp.stack([own_pair, swap(own_pair, "j")])
    came, own_four, mixed_pair = lax.optimization_barrier((came, own_four, mixed_pair))
    rows_z = jnp.concatenate([b[0] for b in came], axis=0)
    grads_z = jnp.concatenate([b[1] for b in came], axis=0)
    count = experts * cap

    rows_x, grads_y = lax.optimization_barrier((swap(rows_z, "x"), swap(grads_z, "j")))
    rows_pair = jnp.stack([rows_z, rows_x])
    grads_pair = jnp.stack([grads_z, grads_y])
    own_sib = swap(own_four, "c")
    mixed_rel = [mixed_pair] + exchange([mixed_pair] * experts, 1)
    rows_y, grads_x, own_sib, mixed_rel = lax.optimization_barrier(
        (swap(rows_pair, "j"), swap(grads_pair, "x"), own_sib, mixed_rel)
    )
    rows_four = jnp.stack([rows_pair, rows_y])
    grads_four = jnp.stack([grads_pair, grads_x], axis=1)
    rows_sib, grads_sib = swap(rows_four, "c"), swap(grads_four, "c")

    def assemble(which, four, sib):
        cells = []
        for own, rest in ((own_four, four), (own_sib, sib)):
            for dx in range(2):
                cells.append(jnp.concatenate([own[:, dx, which], rest[:, dx]], axis=1))
        return jnp.concatenate(cells, axis=-1).reshape(2 * count, features)

    rows = assemble(0, rows_four, rows_sib)
    grads = assemble(1, grads_four, grads_sib)

    gate_w = jnp.concatenate(relative(w_gate[0], 0, place), axis=0)
    up_w = jnp.concatenate(relative(w_up[0], 0, place), axis=0)
    down_w = jnp.concatenate(relative(w_down[0], 1, place), axis=1)
    pre_gate = dot(rows, gate_w, 1, 0)
    pre_up = dot(rows, up_w, 1, 0)
    sigmoid_gate = jax.nn.sigmoid(pre_gate)
    activated = pre_gate * sigmoid_gate
    hidden = (activated * pre_up).astype(BF16)
    d_hidden = dot(grads, down_w, 1, 1)
    d_gate = (d_hidden * pre_up * sigmoid_gate * (1.0 + pre_gate * (1.0 - sigmoid_gate))).astype(
        BF16
    )
    d_up = (d_hidden * activated).astype(BF16)

    split = features // 2
    away = dot(d_gate, gate_w[split:], 1, 1) + dot(d_up, up_w[split:], 1, 1)
    other = swap(away.astype(BF16), "c")
    kept = dot(d_gate, gate_w[:split], 1, 1) + dot(d_up, up_w[:split], 1, 1)
    total = (kept + other.astype(F32)).astype(BF16)
    block = lambda dj, dx: total[dj * count : (dj + 1) * count, dx * quarter : (dx + 1) * quarter]
    summed = (
        block(0, 0).astype(F32)
        + swap(block(0, 1), "x").astype(F32)
        + swap(block(1, 0), "j").astype(F32)
        + swap_both(block(1, 1)).astype(F32)
    ).astype(BF16)
    back = [summed[s * cap : (s + 1) * cap] for s in range(experts)]
    back = back[:1] + exchange(back, -1)

    grad_up = dot(rows, d_up, 0, 0).astype(BF16)
    grad_down = dot(hidden, grads, 0, 0).astype(BF16)
    grad_up, grad_down = absolute(grad_up, 0, place), absolute(grad_down, 1, place)

    d_part = dot(
        sel.reshape(experts * cap, tokens), jnp.concatenate(back, axis=0), 0, 0
    ).astype(BF16)
    d_normed = lax.all_gather(d_part, ("x", "c"), axis=1, tiled=True).astype(F32)
    resid_f32 = residual.astype(F32)
    inv_rms = lax.rsqrt(jnp.mean(resid_f32 * resid_f32, axis=-1, keepdims=True) + epsilon)
    unit_rows = resid_f32 * inv_rms
    row_mean = jnp.mean(unit_rows * d_normed, axis=-1, keepdims=True)
    grad_resid = (out_grad.astype(F32) + inv_rms * (d_normed - unit_rows * row_mean)).astype(BF16)

    mixed_rel = jnp.stack(mixed_rel)
    channels = mixed.shape[1]
    mixed_rel = mixed_rel.reshape(slices, tokens, channels)
    mixed_all = jnp.concatenate(
        [
            lax.dynamic_slice_in_dim(
                mixed_rel, lax.rem(mine - e + experts, experts) * 2 + (half ^ j), 1, 0
            )
            for e in range(experts)
            for j in range(2)
        ],
        axis=0,
    )
    part = tokens // 2
    ordered = [
        lax.dynamic_slice_in_dim(mixed_all, (core ^ d) * part, part, 1).reshape(-1, channels)
        for d in range(2)
    ]
    width = features // slices
    mine_rows = lax.dynamic_slice_in_dim(grad_resid, core * part, part, 0)
    blocks = jnp.transpose(mine_rows.reshape(part, slices, width), (1, 0, 2))
    got = lax.all_to_all(blocks, ("e", "j"), 0, 0, tiled=True).reshape(slices * part, width)
    got_sib = swap(got, "c")
    grad_w_out = dot(got, ordered[0], 0, 0) + dot(got_sib, ordered[1], 0, 0)

    d_mix = dot(grad_resid, w_out, 1, 1)
    grad_out_gate = (d_mix * conv_f32).astype(BF16)
    d_conv = d_mix * gate_f32
    edge = d_conv.astype(BF16)
    ends = slices - 1
    above = lax.ppermute(edge[-1:], ("e", "j"), [(i, i + 1) for i in range(ends)]).astype(F32)
    below = lax.ppermute(edge[:1], ("e", "j"), [(i + 1, i) for i in range(ends)]).astype(F32)
    later = jnp.concatenate([d_conv[1:], below], axis=0)
    earlier = jnp.concatenate([above, d_conv[:-1]], axis=0)
    d_inner = conv_taps[0] * later + conv_taps[1] * d_conv + conv_taps[2] * earlier
    grad_in_gate = (d_inner * conv_input.astype(F32)).astype(BF16)
    grad_conv_input = (d_inner * in_gate.astype(F32)).astype(BF16)
    return (
        grad_resid,
        grad_up[None],
        grad_down[None],
        grad_out_gate,
        grad_in_gate,
        grad_conv_input,
        grad_w_out,
    )


def solution(mesh):
    slices, blocks = mesh.shape["sp"], mesh.shape["tp"]
    grid = mesh.devices.reshape(slices // 2, 2, blocks // 2, 2)
    inner = Mesh(grid, ("e", "j", "x", "c"))
    sp, tp = ("e", "j"), ("x", "c")
    in_specs = (
        P(sp, None),
        P(sp, None),
        P(sp, None),
        P(sp, None),
        P(sp, None, tp),
        P(sp, None, tp),
        P(sp, tp, None),
        P(sp, tp),
        P(sp, tp),
        P(sp, tp),
        P(sp, tp),
        P(None, tp),
        P(tp, None),
    )
    out_specs = (
        P(sp, None),
        P(sp, None, tp),
        P(sp, tp, None),
        P(sp, tp),
        P(sp, tp),
        P(sp, tp),
        P(sp, tp),
    )

    return jax.shard_map(
        per_device, mesh=inner, in_specs=in_specs, out_specs=out_specs, check_vma=False
    )
```

```python
import functools

import jax
import jax.numpy as jnp
from jax import lax
from jax.experimental import pallas as pl
from jax.experimental.pallas import tpu as pltpu
from jax.sharding import Mesh
from jax.sharding import PartitionSpec as P


epsilon = 1e-06
F32 = jnp.float32
BF16 = jnp.bfloat16
LIMIT = 8 * 2**20


def swap(value, axis):
    return lax.ppermute(value, axis, [(0, 1), (1, 0)])


def swap_both(value):
    return lax.ppermute(value, ("j", "x"), [(i, 3 - i) for i in range(4)])


def exchange(blocks, sign):
    count = lax.axis_size("e")
    if count <= 8:
        return [
            lax.ppermute(b, "e", [(i, (i + sign * s) % count) for i in range(count)])
            for s, b in enumerate(blocks)
            if s
        ]
    mine, order = lax.axis_index("e"), jnp.arange(count)
    to = jnp.take(jnp.stack(blocks), sign * (order - mine) % count, axis=0)
    came = lax.all_to_all(to, "e", 0, 0, tiled=True)
    came = jnp.take(came, (mine - sign * order) % count, axis=0)
    return [came[s] for s in range(1, count)]


def dot(a, b, ca, cb):
    return lax.dot_general(a, b, (((ca,), (cb,)), ((), ())), preferred_element_type=F32)


def prepare(experts, cap, quarter, index_ref, routes_ref, weights_ref, resid_ref, grad_ref, *outs):
    sends, sel_ref = outs[:-1], outs[-1]
    tokens = resid_ref.shape[0]
    mine, column = index_ref[0], index_ref[1]
    resid = resid_ref[...].astype(F32)
    inv_rms = lax.rsqrt(jnp.mean(resid * resid, axis=-1, keepdims=True) + epsilon)
    cols = pl.ds(pl.multiple_of(column * quarter, quarter), quarter)
    normed = (resid_ref[:, cols].astype(F32) * inv_rms).astype(BF16)
    grad = grad_ref[:, cols]
    first, second = routes_ref[0:1, :], routes_ref[1:2, :]
    first = jnp.where(first >= mine, first - mine, first - mine + experts)
    second = jnp.where(second >= mine, second - mine, second - mine + experts)
    ids = lax.broadcasted_iota(jnp.int32, (experts, tokens), 0)
    in_first, in_second = ids == first, ids == second
    member = jnp.where(in_first | in_second, 1.0, 0.0)
    before = jnp.where(
        lax.broadcasted_iota(jnp.int32, (tokens, tokens), 0)
        < lax.broadcasted_iota(jnp.int32, (tokens, tokens), 1),
        1.0,
        0.0,
    )
    rank = dot(member.astype(BF16), before.astype(BF16), 1, 0)
    rank_first = jnp.sum(jnp.where(in_first, rank, 0.0), axis=0, keepdims=True).astype(jnp.int32)
    rank_second = jnp.sum(jnp.where(in_second, rank, 0.0), axis=0, keepdims=True).astype(jnp.int32)
    slot_first = first * cap + rank_first
    slot_second = second * cap + rank_second
    for step in range(experts):
        slots = lax.broadcasted_iota(jnp.int32, (cap, tokens), 0) + step * cap
        hit_first, hit_second = slots == slot_first, slots == slot_second
        pick = jnp.where(hit_first | hit_second, 1.0, 0.0).astype(BF16)
        share = jnp.where(hit_first, weights_ref[0:1, :], 0.0) + jnp.where(
            hit_second, weights_ref[1:2, :], 0.0
        )
        share = jnp.sum(share, axis=1, keepdims=True)
        sel_ref[step] = pick
        sends[step][0] = dot(pick, normed, 1, 0).astype(BF16)
        sends[step][1] = (share * dot(pick, grad, 1, 0)).astype(BF16)


def columns(place, step, width):
    return pl.ds(pl.multiple_of((place ^ step) * width, width), width)


def first_half(
    cap,
    place_ref,
    own_ref,
    own_sib_ref,
    own_y_ref,
    own_y_sib_ref,
    pair_ref,
    pair_sib_ref,
    near_own_ref,
    near_own_sib_ref,
    near_ref,
    near_sib_ref,
    gate_ref,
    up_ref,
    down_ref,
    rows_ref,
    pre_gate_ref,
    pre_up_ref,
    near_out_ref,
    half_ref,
):
    place = place_ref[0]
    quarter = pair_ref.shape[-1]
    count = cap + pair_ref.shape[1]
    sides = (
        (own_ref, own_y_ref, pair_ref, near_own_ref, near_ref),
        (own_sib_ref, own_y_sib_ref, pair_sib_ref, near_own_sib_ref, near_sib_ref),
    )
    for dc, (own, own_y, pair, near_own, near) in enumerate(sides):
        for dx in range(2):
            cols = columns(place, 2 * dx + dc, quarter)
            rows_ref[:cap, cols] = own[dx * cap : (dx + 1) * cap]
            rows_ref[cap:count, cols] = pair[dx]
            rows_ref[count:, cols] = own_y[dx * cap : (dx + 1) * cap]
        cols = slice(dc * quarter, (dc + 1) * quarter)
        for dj in range(2):
            near_out_ref[dj * count : dj * count + cap, cols] = near_own[dj]
            near_out_ref[dj * count + cap : (dj + 1) * count, cols] = near[dj]
    rows = rows_ref[...]
    pre_gate_ref[...] = dot(rows, gate_ref[...], 1, 0)
    pre_up_ref[...] = dot(rows, up_ref[...], 1, 0)
    half_ref[...] = dot(
        near_out_ref[:, :quarter], down_ref[:, columns(place, 0, quarter)], 1, 1
    ) + dot(near_out_ref[:, quarter:], down_ref[:, columns(place, 1, quarter)], 1, 1)


def second_half(
    cap,
    place_ref,
    rows_y_ref,
    rows_y_sib_ref,
    far_own_ref,
    far_own_sib_ref,
    far_ref,
    far_sib_ref,
    pre_gate_ref,
    pre_up_ref,
    half_ref,
    gate_ref,
    up_ref,
    down_ref,
    rows_ref,
    far_out_ref,
    hidden_ref,
    d_gate_ref,
    d_up_ref,
    away_ref,
    late_gate_ref,
    late_up_ref,
):
    place = place_ref[0]
    quarter = far_ref.shape[-1]
    count = cap + far_ref.shape[1]
    early = pre_gate_ref.shape[0]
    sides = ((rows_y_ref, far_own_ref, far_ref), (rows_y_sib_ref, far_own_sib_ref, far_sib_ref))
    for dc, (rows_y, far_own, far) in enumerate(sides):
        for dx in range(2):
            rows_ref[:, columns(place, 2 * dx + dc, quarter)] = rows_y[dx]
        cols = slice(dc * quarter, (dc + 1) * quarter)
        for dj in range(2):
            far_out_ref[dj * count : dj * count + cap, cols] = far_own[dj]
            far_out_ref[dj * count + cap : (dj + 1) * count, cols] = far[dj]
    rows = rows_ref[...]
    late_gate_ref[...] = dot(rows, gate_ref[...], 1, 0)
    late_up_ref[...] = dot(rows, up_ref[...], 1, 0)
    for low, high, gate_at, up_at in (
        (0, early, pre_gate_ref, pre_up_ref),
        (early, 2 * count, late_gate_ref, late_up_ref),
    ):
        part = slice(low, high)
        d_hidden = half_ref[part] + (
            dot(far_out_ref[part, :quarter], down_ref[:, columns(place, 2, quarter)], 1, 1)
            + dot(far_out_ref[part, quarter:], down_ref[:, columns(place, 3, quarter)], 1, 1)
        )
        pre_gate, pre_up = gate_at[...], up_at[...]
        sigmoid_gate = jax.nn.sigmoid(pre_gate)
        activated = pre_gate * sigmoid_gate
        hidden_ref[part] = (activated * pre_up).astype(BF16)
        d_gate_ref[part] = (
            d_hidden * pre_up * sigmoid_gate * (1.0 + pre_gate * (1.0 - sigmoid_gate))
        ).astype(BF16)
        d_up_ref[part] = (d_hidden * activated).astype(BF16)
    for dx in range(2):
        block = columns(place, 2 * dx + 1, quarter)
        away_ref[:, dx * quarter : (dx + 1) * quarter] = (
            dot(d_gate_ref[...], gate_ref[block], 1, 1) + dot(d_up_ref[...], up_ref[block], 1, 1)
        ).astype(BF16)


def in_vmem(kernel, outs, scratch, flops, scalars, *values):
    vmem = pl.BlockSpec(memory_space=pltpu.VMEM)
    return pl.pallas_call(
        kernel,
        out_shape=[jax.ShapeDtypeStruct(shape, kind) for shape, kind in outs],
        in_specs=[pl.BlockSpec(memory_space=pltpu.SMEM)] + [vmem] * len(values),
        out_specs=[vmem] * len(outs),
        scratch_shapes=scratch,
        cost_estimate=pl.CostEstimate(flops=flops, bytes_accessed=0, transcendentals=0),
        compiler_params=pltpu.CompilerParams(vmem_limit_bytes=LIMIT),
    )(scalars, *[pltpu.with_memory_space_constraint(v, pltpu.VMEM) for v in values])


def absolute(value, axis, place):
    width = value.shape[axis] // 4
    return jnp.concatenate(
        [lax.dynamic_slice_in_dim(value, (place ^ q) * width, width, axis) for q in range(4)],
        axis=axis,
    )


def per_device(
    out_grad,
    residual,
    routes,
    route_weights,
    w_gate,
    w_up,
    w_down,
    out_gate,
    in_gate,
    conv_input,
    conv_out,
    conv_taps,
    w_out,
):
    tokens, features = out_grad.shape
    experts = lax.axis_size("e")
    slices = 2 * experts
    cap = -(-(5 * tokens // slices) // 16) * 16
    quarter = features // 4
    mine, half, core = lax.axis_index("e"), lax.axis_index("j"), lax.axis_index("c")
    place = 2 * lax.axis_index("x") + core
    index = jnp.stack([mine, place]).astype(jnp.int32)

    outs = in_vmem(
        functools.partial(prepare, experts, cap, quarter),
        [((2, cap, quarter), BF16)] * experts + [((experts, cap, tokens), BF16)],
        [],
        4 * experts * cap * tokens * quarter,
        index,
        routes.T,
        route_weights.T,
        residual,
        out_grad,
    )
    sends, sel = outs[:-1], outs[-1]
    conv_f32 = conv_out.astype(F32)
    gate_f32 = out_gate.astype(F32)
    mixed = (gate_f32 * conv_f32).astype(BF16)
    channels = mixed.shape[1]
    fold = quarter // channels
    mixed_rows = tokens // fold
    mixed_wide = jnp.concatenate(
        [mixed[i * mixed_rows : (i + 1) * mixed_rows] for i in range(fold)], axis=1
    )

    came = exchange(sends, 1)
    own_rows, own_grads = sends[0][0], sends[0][1]
    own_rows_x, own_grads_y = lax.optimization_barrier((swap(own_rows, "x"), swap(own_grads, "j")))
    own_pair = jnp.concatenate([own_rows, own_rows_x, mixed_wide], axis=0)
    own_near = jnp.stack([own_grads, own_grads_y])
    own_y = swap(own_pair, "j")
    own_far = swap(own_near, "x")
    came = lax.optimization_barrier(came)
    rows_z = jnp.concatenate([b[0] for b in came], axis=0)
    grads_z = jnp.concatenate([b[1] for b in came], axis=0)
    count = experts * cap

    rows_x, grads_y, own_y, own_far = lax.optimization_barrier(
        (swap(rows_z, "x"), swap(grads_z, "j"), own_y, own_far)
    )
    pair = jnp.stack([rows_z, rows_x])
    near = jnp.stack([grads_z, grads_y])
    own_far_sib = swap(own_far, "c")
    rows_y, far, own_far_sib = lax.optimization_barrier(
        (swap(pair, "j"), swap(near, "x"), own_far_sib)
    )
    weights = (w_gate[0], w_up[0], w_down[0])
    hidden_units = weights[0].shape[1]
    early = count + cap
    here = place.reshape(1).astype(jnp.int32)
    sib = lambda value: (value, swap(value, "c"))
    rows_early, pre_gate, pre_up, grads_near, d_half = in_vmem(
        functools.partial(first_half, cap),
        [
            ((early, features), BF16),
            ((early, hidden_units), F32),
            ((early, hidden_units), F32),
            ((2 * count, features // 2), BF16),
            ((2 * count, hidden_units), F32),
        ],
        [],
        (4 * early + 2 * count) * features * hidden_units,
        here,
        *sib(own_pair),
        *sib(own_y),
        *sib(pair),
        *sib(own_near),
        *sib(near),
        *weights,
    )
    rows_late, grads_far, hidden, d_gate, d_up, away = in_vmem(
        functools.partial(second_half, cap),
        [
            ((2 * count - early, features), BF16),
            ((2 * count, features // 2), BF16),
            ((2 * count, hidden_units), BF16),
            ((2 * count, hidden_units), BF16),
            ((2 * count, hidden_units), BF16),
            ((2 * count, features // 2), BF16),
        ],
        [pltpu.VMEM((2 * count - early, hidden_units), F32)] * 2,
        (4 * (2 * count - early) + 6 * count) * features * hidden_units,
        here,
        *sib(rows_y),
        own_far,
        own_far_sib,
        *sib(far),
        pre_gate,
        pre_up,
        d_half,
        *weights,
    )

    keep = lambda value: jnp.concatenate(
        [
            lax.dynamic_slice_in_dim(value, (place ^ (2 * dx)) * quarter, quarter, 0)
            for dx in range(2)
        ],
        axis=0,
    )
    other = swap(away, "c")
    kept = dot(d_gate, keep(weights[0]), 1, 1) + dot(d_up, keep(weights[1]), 1, 1)
    total = (kept + other.astype(F32)).astype(BF16)
    block = lambda dj, dx: total[dj * count : (dj + 1) * count, dx * quarter : (dx + 1) * quarter]
    mixed_mine = jnp.stack([own_pair[2 * cap :], own_y[2 * cap :]])
    mixed_rel = [mixed_mine] + exchange([mixed_mine] * experts, 1)
    summed = (
        block(0, 0).astype(F32)
        + swap(block(0, 1), "x").astype(F32)
        + swap(block(1, 0), "j").astype(F32)
        + swap_both(block(1, 1)).astype(F32)
    ).astype(BF16)
    summed, mixed_rel = lax.optimization_barrier((summed, mixed_rel))
    back = [summed[s * cap : (s + 1) * cap] for s in range(experts)]
    back = back[:1] + exchange(back, -1)

    grad_up = (dot(rows_early, d_up[:early], 0, 0) + dot(rows_late, d_up[early:], 0, 0)).astype(
        BF16
    )
    down_near = dot(hidden, grads_near, 0, 0).astype(BF16)
    down_far = dot(hidden, grads_far, 0, 0).astype(BF16)
    grad_down = absolute(jnp.concatenate([down_near, down_far], axis=1), 1, place)

    d_part = dot(
        sel.reshape(experts * cap, tokens), jnp.concatenate(back, axis=0), 0, 0
    ).astype(BF16)
    d_normed = lax.all_gather(d_part, ("x", "c"), axis=1, tiled=True).astype(F32)
    resid_f32 = residual.astype(F32)
    inv_rms = lax.rsqrt(jnp.mean(resid_f32 * resid_f32, axis=-1, keepdims=True) + epsilon)
    unit_rows = resid_f32 * inv_rms
    row_mean = jnp.mean(unit_rows * d_normed, axis=-1, keepdims=True)
    grad_resid = (out_grad.astype(F32) + inv_rms * (d_normed - unit_rows * row_mean)).astype(BF16)

    mixed_rel = jnp.stack(mixed_rel).reshape(slices, mixed_rows, fold, channels)
    mixed_rel = jnp.concatenate([mixed_rel[:, :, i] for i in range(fold)], axis=1)
    mixed_all = jnp.concatenate(
        [
            lax.dynamic_slice_in_dim(
                mixed_rel, lax.rem(mine - e + experts, experts) * 2 + (half ^ j), 1, 0
            )
            for e in range(experts)
            for j in range(2)
        ],
        axis=0,
    )
    part = tokens // 2
    ordered = [
        lax.dynamic_slice_in_dim(mixed_all, (core ^ d) * part, part, 1).reshape(-1, channels)
        for d in range(2)
    ]
    width = features // slices
    mine_rows = lax.dynamic_slice_in_dim(grad_resid, core * part, part, 0)
    blocks = jnp.transpose(mine_rows.reshape(part, slices, width), (1, 0, 2))
    got = lax.all_to_all(blocks, ("e", "j"), 0, 0, tiled=True).reshape(slices * part, width)
    got_sib = swap(got, "c")
    grad_w_out = dot(got, ordered[0], 0, 0) + dot(got_sib, ordered[1], 0, 0)

    d_mix = dot(grad_resid, w_out, 1, 1)
    grad_out_gate = (d_mix * conv_f32).astype(BF16)
    d_conv = d_mix * gate_f32
    edge = d_conv.astype(BF16)
    ends = slices - 1
    above = lax.ppermute(edge[-1:], ("e", "j"), [(i, i + 1) for i in range(ends)]).astype(F32)
    below = lax.ppermute(edge[:1], ("e", "j"), [(i + 1, i) for i in range(ends)]).astype(F32)
    later = jnp.concatenate([d_conv[1:], below], axis=0)
    earlier = jnp.concatenate([above, d_conv[:-1]], axis=0)
    d_inner = conv_taps[0] * later + conv_taps[1] * d_conv + conv_taps[2] * earlier
    grad_in_gate = (d_inner * conv_input.astype(F32)).astype(BF16)
    grad_conv_input = (d_inner * in_gate.astype(F32)).astype(BF16)
    return (
        grad_resid,
        grad_up[None],
        grad_down[None],
        grad_out_gate,
        grad_in_gate,
        grad_conv_input,
        grad_w_out,
    )


def solution(mesh):
    slices, blocks = mesh.shape["sp"], mesh.shape["tp"]
    grid = mesh.devices.reshape(slices // 2, 2, blocks // 2, 2)
    inner = Mesh(grid, ("e", "j", "x", "c"))
    sp, tp = ("e", "j"), ("x", "c")
    in_specs = (
        P(sp, None),
        P(sp, None),
        P(sp, None),
        P(sp, None),
        P(sp, None, tp),
        P(sp, None, tp),
        P(sp, tp, None),
        P(sp, tp),
        P(sp, tp),
        P(sp, tp),
        P(sp, tp),
        P(None, tp),
        P(tp, None),
    )
    out_specs = (
        P(sp, None),
        P(sp, None, tp),
        P(sp, tp, None),
        P(sp, tp),
        P(sp, tp),
        P(sp, tp),
        P(sp, tp),
    )

    return jax.shard_map(
        per_device, mesh=inner, in_specs=in_specs, out_specs=out_specs, check_vma=False
    )
```

```python
import functools

import jax
import jax.numpy as jnp
from jax import lax
from jax.experimental import pallas as pl
from jax.experimental.pallas import tpu as pltpu
from jax.sharding import Mesh
from jax.sharding import PartitionSpec as P


epsilon = 1e-06
F32 = jnp.float32
BF16 = jnp.bfloat16


def swap(value, axis):
    return lax.ppermute(value, axis, [(0, 1), (1, 0)])


def swap_both(value):
    return lax.ppermute(value, ("j", "x"), [(i, 3 - i) for i in range(4)])


def exchange(blocks, sign):
    count = lax.axis_size("e")
    if count <= 8:
        return [
            lax.ppermute(b, "e", [(i, (i + sign * s) % count) for i in range(count)])
            for s, b in enumerate(blocks)
            if s
        ]
    mine, order = lax.axis_index("e"), jnp.arange(count)
    to = jnp.take(jnp.stack(blocks), sign * (order - mine) % count, axis=0)
    came = lax.all_to_all(to, "e", 0, 0, tiled=True)
    came = jnp.take(came, (mine - sign * order) % count, axis=0)
    return [came[s] for s in range(1, count)]


def dot(a, b, ca, cb):
    return lax.dot_general(a, b, (((ca,), (cb,)), ((), ())), preferred_element_type=F32)


def prepare(experts, cap, quarter, index_ref, routes_ref, weights_ref, resid_ref, grad_ref, *outs):
    sends, sel_ref = outs[:-1], outs[-1]
    tokens = resid_ref.shape[0]
    mine, column = index_ref[0], index_ref[1]
    resid = resid_ref[...].astype(F32)
    inv_rms = lax.rsqrt(jnp.mean(resid * resid, axis=-1, keepdims=True) + epsilon)
    cols = pl.ds(pl.multiple_of(column * quarter, quarter), quarter)
    normed = (resid_ref[:, cols].astype(F32) * inv_rms).astype(BF16)
    grad = grad_ref[:, cols]
    first, second = routes_ref[0:1, :], routes_ref[1:2, :]
    first = jnp.where(first >= mine, first - mine, first - mine + experts)
    second = jnp.where(second >= mine, second - mine, second - mine + experts)
    ids = lax.broadcasted_iota(jnp.int32, (experts, tokens), 0)
    in_first, in_second = ids == first, ids == second
    member = jnp.where(in_first | in_second, 1.0, 0.0)
    before = jnp.where(
        lax.broadcasted_iota(jnp.int32, (tokens, tokens), 0)
        < lax.broadcasted_iota(jnp.int32, (tokens, tokens), 1),
        1.0,
        0.0,
    )
    rank = dot(member.astype(BF16), before.astype(BF16), 1, 0)
    rank_first = jnp.sum(jnp.where(in_first, rank, 0.0), axis=0, keepdims=True).astype(jnp.int32)
    rank_second = jnp.sum(jnp.where(in_second, rank, 0.0), axis=0, keepdims=True).astype(jnp.int32)
    slot_first = first * cap + rank_first
    slot_second = second * cap + rank_second
    for step in range(experts):
        slots = lax.broadcasted_iota(jnp.int32, (cap, tokens), 0) + step * cap
        hit_first, hit_second = slots == slot_first, slots == slot_second
        pick = jnp.where(hit_first | hit_second, 1.0, 0.0).astype(BF16)
        share = jnp.where(hit_first, weights_ref[0:1, :], 0.0) + jnp.where(
            hit_second, weights_ref[1:2, :], 0.0
        )
        share = jnp.sum(share, axis=1, keepdims=True)
        sel_ref[step] = pick
        sends[step][0] = dot(pick, normed, 1, 0).astype(BF16)
        sends[step][1] = (share * dot(pick, grad, 1, 0)).astype(BF16)


def columns(place, step, width):
    return pl.ds(pl.multiple_of((place ^ step) * width, width), width)


def first_half(
    cap,
    place_ref,
    own_ref,
    own_sib_ref,
    own_y_ref,
    own_y_sib_ref,
    pair_ref,
    pair_sib_ref,
    near_own_ref,
    near_own_sib_ref,
    near_ref,
    near_sib_ref,
    gate_ref,
    up_ref,
    down_ref,
    rows_ref,
    pre_gate_ref,
    pre_up_ref,
    near_out_ref,
    half_ref,
):
    place = place_ref[0]
    quarter = pair_ref.shape[-1]
    count = cap + pair_ref.shape[1]
    sides = (
        (own_ref, own_y_ref, pair_ref, near_own_ref, near_ref),
        (own_sib_ref, own_y_sib_ref, pair_sib_ref, near_own_sib_ref, near_sib_ref),
    )
    for dc, (own, own_y, pair, near_own, near) in enumerate(sides):
        for dx in range(2):
            cols = columns(place, 2 * dx + dc, quarter)
            rows_ref[:cap, cols] = own[dx * cap : (dx + 1) * cap]
            rows_ref[cap:count, cols] = pair[dx]
            rows_ref[count:, cols] = own_y[dx * cap : (dx + 1) * cap]
        cols = slice(dc * quarter, (dc + 1) * quarter)
        for dj in range(2):
            near_out_ref[dj * count : dj * count + cap, cols] = near_own[dj]
            near_out_ref[dj * count + cap : (dj + 1) * count, cols] = near[dj]
    rows = rows_ref[...]
    pre_gate_ref[...] = dot(rows, gate_ref[...], 1, 0)
    pre_up_ref[...] = dot(rows, up_ref[...], 1, 0)
    half_ref[...] = dot(
        near_out_ref[:, :quarter], down_ref[:, columns(place, 0, quarter)], 1, 1
    ) + dot(near_out_ref[:, quarter:], down_ref[:, columns(place, 1, quarter)], 1, 1)


def second_half(
    cap,
    place_ref,
    rows_y_ref,
    rows_y_sib_ref,
    far_own_ref,
    far_own_sib_ref,
    far_ref,
    far_sib_ref,
    pre_gate_ref,
    pre_up_ref,
    half_ref,
    gate_ref,
    up_ref,
    down_ref,
    rows_ref,
    far_out_ref,
    hidden_ref,
    d_gate_ref,
    d_up_ref,
    away_ref,
    late_gate_ref,
    late_up_ref,
):
    place = place_ref[0]
    quarter = far_ref.shape[-1]
    count = cap + far_ref.shape[1]
    early = pre_gate_ref.shape[0]
    sides = ((rows_y_ref, far_own_ref, far_ref), (rows_y_sib_ref, far_own_sib_ref, far_sib_ref))
    for dc, (rows_y, far_own, far) in enumerate(sides):
        for dx in range(2):
            rows_ref[:, columns(place, 2 * dx + dc, quarter)] = rows_y[dx]
        cols = slice(dc * quarter, (dc + 1) * quarter)
        for dj in range(2):
            far_out_ref[dj * count : dj * count + cap, cols] = far_own[dj]
            far_out_ref[dj * count + cap : (dj + 1) * count, cols] = far[dj]
    rows = rows_ref[...]
    late_gate_ref[...] = dot(rows, gate_ref[...], 1, 0)
    late_up_ref[...] = dot(rows, up_ref[...], 1, 0)
    for low, high, gate_at, up_at in (
        (0, early, pre_gate_ref, pre_up_ref),
        (early, 2 * count, late_gate_ref, late_up_ref),
    ):
        part = slice(low, high)
        d_hidden = half_ref[part] + (
            dot(far_out_ref[part, :quarter], down_ref[:, columns(place, 2, quarter)], 1, 1)
            + dot(far_out_ref[part, quarter:], down_ref[:, columns(place, 3, quarter)], 1, 1)
        )
        pre_gate, pre_up = gate_at[...], up_at[...]
        sigmoid_gate = jax.nn.sigmoid(pre_gate)
        activated = pre_gate * sigmoid_gate
        hidden_ref[part] = (activated * pre_up).astype(BF16)
        d_gate_ref[part] = (
            d_hidden * pre_up * sigmoid_gate * (1.0 + pre_gate * (1.0 - sigmoid_gate))
        ).astype(BF16)
        d_up_ref[part] = (d_hidden * activated).astype(BF16)
    for dx in range(2):
        block = columns(place, 2 * dx + 1, quarter)
        away_ref[:, dx * quarter : (dx + 1) * quarter] = (
            dot(d_gate_ref[...], gate_ref[block], 1, 1) + dot(d_up_ref[...], up_ref[block], 1, 1)
        ).astype(BF16)


def finish(core_ref, d_normed_ref, resid_ref, grad_ref, out_ref, blocks_ref):
    d_normed = d_normed_ref[...].astype(F32)
    resid = resid_ref[...].astype(F32)
    inv_rms = lax.rsqrt(jnp.mean(resid * resid, axis=-1, keepdims=True) + epsilon)
    unit = resid * inv_rms
    row_mean = jnp.mean(unit * d_normed, axis=-1, keepdims=True)
    out_ref[...] = (
        grad_ref[...].astype(F32) + inv_rms * (d_normed - unit * row_mean)
    ).astype(BF16)
    count, part, width = blocks_ref.shape
    mine = pl.ds(pl.multiple_of(core_ref[0] * part, part), part)
    for s in range(count):
        blocks_ref[s] = out_ref[mine, s * width : (s + 1) * width]


def in_vmem(kernel, outs, scratch, flops, limit, scalars, *values):
    vmem = pl.BlockSpec(memory_space=pltpu.VMEM)
    return pl.pallas_call(
        kernel,
        out_shape=[jax.ShapeDtypeStruct(shape, kind) for shape, kind in outs],
        in_specs=[pl.BlockSpec(memory_space=pltpu.SMEM)] + [vmem] * len(values),
        out_specs=[vmem] * len(outs),
        scratch_shapes=scratch,
        cost_estimate=pl.CostEstimate(flops=flops, bytes_accessed=0, transcendentals=0),
        compiler_params=pltpu.CompilerParams(vmem_limit_bytes=limit),
    )(scalars, *values)


def absolute(value, axis, place):
    width = value.shape[axis] // 4
    return jnp.concatenate(
        [lax.dynamic_slice_in_dim(value, (place ^ q) * width, width, axis) for q in range(4)],
        axis=axis,
    )


def per_device(
    out_grad,
    residual,
    routes,
    route_weights,
    w_gate,
    w_up,
    w_down,
    out_gate,
    in_gate,
    conv_input,
    conv_out,
    conv_taps,
    w_out,
):
    tokens, features = out_grad.shape
    experts = lax.axis_size("e")
    slices = 2 * experts
    cap = -(-(5 * tokens // slices) // 16) * 16
    quarter = features // 4
    mine, half, core = lax.axis_index("e"), lax.axis_index("j"), lax.axis_index("c")
    place = 2 * lax.axis_index("x") + core
    index = jnp.stack([mine, place]).astype(jnp.int32)

    outs = in_vmem(
        functools.partial(prepare, experts, cap, quarter),
        [((2, cap, quarter), BF16)] * experts + [((experts, cap, tokens), BF16)],
        [],
        4 * experts * cap * tokens * quarter,
        60 * 2**20,
        index,
        routes.T,
        route_weights.T,
        residual,
        out_grad,
    )
    sends, sel = outs[:-1], outs[-1]
    conv_f32 = conv_out.astype(F32)
    gate_f32 = out_gate.astype(F32)
    mixed = (gate_f32 * conv_f32).astype(BF16)
    channels = mixed.shape[1]
    fold = quarter // channels
    mixed_rows = tokens // fold
    mixed_wide = jnp.concatenate(
        [mixed[i * mixed_rows : (i + 1) * mixed_rows] for i in range(fold)], axis=1
    )

    came = exchange(sends, 1)
    own_rows, own_grads = sends[0][0], sends[0][1]
    own_rows_x, own_grads_y = lax.optimization_barrier((swap(own_rows, "x"), swap(own_grads, "j")))
    own_pair = jnp.concatenate([own_rows, own_rows_x, mixed_wide], axis=0)
    own_near = jnp.stack([own_grads, own_grads_y])
    own_y = swap(own_pair, "j")
    own_far = swap(own_near, "x")
    came = lax.optimization_barrier(came)
    rows_z = jnp.concatenate([b[0] for b in came], axis=0)
    grads_z = jnp.concatenate([b[1] for b in came], axis=0)
    count = experts * cap

    rows_x, grads_y, own_y, own_far = lax.optimization_barrier(
        (swap(rows_z, "x"), swap(grads_z, "j"), own_y, own_far)
    )
    pair = jnp.stack([rows_z, rows_x])
    near = jnp.stack([grads_z, grads_y])
    own_far_sib = swap(own_far, "c")
    mixed_mine = jnp.stack([own_pair[2 * cap :], own_y[2 * cap :]])
    mixed_rel = [mixed_mine] + exchange([mixed_mine] * experts, 1)
    rows_y, far, own_far_sib, mixed_rel = lax.optimization_barrier(
        (swap(pair, "j"), swap(near, "x"), own_far_sib, mixed_rel)
    )
    weights = (w_gate[0], w_up[0], w_down[0])
    hidden_units = weights[0].shape[1]
    early = count + cap
    grant = 7 * 4 * 2 * count * hidden_units
    here = place.reshape(1).astype(jnp.int32)
    sib = lambda value: (value, swap(value, "c"))
    rows_early, pre_gate, pre_up, grads_near, d_half = in_vmem(
        functools.partial(first_half, cap),
        [
            ((early, features), BF16),
            ((early, hidden_units), F32),
            ((early, hidden_units), F32),
            ((2 * count, features // 2), BF16),
            ((2 * count, hidden_units), F32),
        ],
        [],
        (4 * early + 2 * count) * features * hidden_units,
        grant,
        here,
        *sib(own_pair),
        *sib(own_y),
        *sib(pair),
        *sib(own_near),
        *sib(near),
        *weights,
    )
    rows_late, grads_far, hidden, d_gate, d_up, away = in_vmem(
        functools.partial(second_half, cap),
        [
            ((2 * count - early, features), BF16),
            ((2 * count, features // 2), BF16),
            ((2 * count, hidden_units), BF16),
            ((2 * count, hidden_units), BF16),
            ((2 * count, hidden_units), BF16),
            ((2 * count, features // 2), BF16),
        ],
        [pltpu.VMEM((2 * count - early, hidden_units), F32)] * 2,
        (4 * (2 * count - early) + 6 * count) * features * hidden_units,
        grant,
        here,
        *sib(rows_y),
        own_far,
        own_far_sib,
        *sib(far),
        pre_gate,
        pre_up,
        d_half,
        *weights,
    )

    keep = lambda value: jnp.concatenate(
        [
            lax.dynamic_slice_in_dim(value, (place ^ (2 * dx)) * quarter, quarter, 0)
            for dx in range(2)
        ],
        axis=0,
    )
    other = swap(away, "c")
    kept = dot(d_gate, keep(weights[0]), 1, 1) + dot(d_up, keep(weights[1]), 1, 1)
    total = (kept + other.astype(F32)).astype(BF16)
    total, mixed_rel = lax.optimization_barrier((total, mixed_rel))
    block = lambda dj, dx: total[dj * count : (dj + 1) * count, dx * quarter : (dx + 1) * quarter]
    summed = (
        block(0, 0).astype(F32)
        + swap(block(0, 1), "x").astype(F32)
        + swap(block(1, 0), "j").astype(F32)
        + swap_both(block(1, 1)).astype(F32)
    ).astype(BF16)
    back = [summed[s * cap : (s + 1) * cap] for s in range(experts)]
    back = back[:1] + exchange(back, -1)

    grad_up = (dot(rows_early, d_up[:early], 0, 0) + dot(rows_late, d_up[early:], 0, 0)).astype(
        BF16
    )
    down_near = dot(hidden, grads_near, 0, 0).astype(BF16)
    down_far = dot(hidden, grads_far, 0, 0).astype(BF16)
    grad_down = absolute(jnp.concatenate([down_near, down_far], axis=1), 1, place)

    d_part = dot(
        sel.reshape(experts * cap, tokens), jnp.concatenate(back, axis=0), 0, 0
    ).astype(BF16)
    d_normed = lax.all_gather(d_part, ("x", "c"), axis=1, tiled=True)
    part = tokens // 2
    width = features // slices
    cut = slices if width % 128 == 0 else 1
    grad_resid, blocks = in_vmem(
        finish,
        [((tokens, features), BF16), ((cut, part, features // cut), BF16)],
        [],
        16 * tokens * features,
        8 * 2**20,
        core.reshape(1).astype(jnp.int32),
        d_normed,
        residual,
        out_grad,
    )

    mixed_rel = jnp.stack(mixed_rel).reshape(slices, mixed_rows, quarter)
    mixed_rel = jnp.concatenate(
        [mixed_rel[:, :, i * channels : (i + 1) * channels] for i in range(fold)], axis=1
    )
    mixed_all = jnp.concatenate(
        [
            lax.dynamic_slice_in_dim(
                mixed_rel, lax.rem(mine - e + experts, experts) * 2 + (half ^ j), 1, 0
            )
            for e in range(experts)
            for j in range(2)
        ],
        axis=0,
    )
    ordered = [
        lax.dynamic_slice_in_dim(mixed_all, (core ^ d) * part, part, 1).reshape(-1, channels)
        for d in range(2)
    ]
    if cut == 1:
        blocks = jnp.transpose(blocks.reshape(part, slices, width), (1, 0, 2))
    got = lax.all_to_all(blocks, ("e", "j"), 0, 0, tiled=True).reshape(slices * part, width)
    got_sib = swap(got, "c")
    grad_w_out = dot(got, ordered[0], 0, 0) + dot(got_sib, ordered[1], 0, 0)

    d_mix = dot(grad_resid, w_out, 1, 1)
    grad_out_gate = (d_mix * conv_f32).astype(BF16)
    d_conv = d_mix * gate_f32
    edge = d_conv.astype(BF16)
    ends = slices - 1
    above = lax.ppermute(edge[-1:], ("e", "j"), [(i, i + 1) for i in range(ends)])
    below = lax.ppermute(edge[:1], ("e", "j"), [(i + 1, i) for i in range(ends)])
    above, below = above.astype(F32), below.astype(F32)
    later = jnp.concatenate([d_conv[1:], below], axis=0)
    earlier = jnp.concatenate([above, d_conv[:-1]], axis=0)
    d_inner = conv_taps[0] * later + conv_taps[1] * d_conv + conv_taps[2] * earlier
    grad_in_gate = (d_inner * conv_input.astype(F32)).astype(BF16)
    grad_conv_input = (d_inner * in_gate.astype(F32)).astype(BF16)
    return (
        grad_resid,
        grad_up[None],
        grad_down[None],
        grad_out_gate,
        grad_in_gate,
        grad_conv_input,
        grad_w_out,
    )


def solution(mesh):
    slices, blocks = mesh.shape["sp"], mesh.shape["tp"]
    grid = mesh.devices.reshape(slices // 2, 2, blocks // 2, 2)
    inner = Mesh(grid, ("e", "j", "x", "c"))
    sp, tp = ("e", "j"), ("x", "c")
    in_specs = (
        P(sp, None),
        P(sp, None),
        P(sp, None),
        P(sp, None),
        P(sp, None, tp),
        P(sp, None, tp),
        P(sp, tp, None),
        P(sp, tp),
        P(sp, tp),
        P(sp, tp),
        P(sp, tp),
        P(None, tp),
        P(tp, None),
    )
    out_specs = (
        P(sp, None),
        P(sp, None, tp),
        P(sp, tp, None),
        P(sp, tp),
        P(sp, tp),
        P(sp, tp),
        P(sp, tp),
    )

    return jax.shard_map(
        per_device, mesh=inner, in_specs=in_specs, out_specs=out_specs, check_vma=False
    )
```

```python
import functools

import jax
import jax.numpy as jnp
from jax import lax
from jax.experimental import pallas as pl
from jax.experimental.pallas import tpu as pltpu
from jax.sharding import Mesh
from jax.sharding import PartitionSpec as P


epsilon = 1e-06
F32 = jnp.float32
BF16 = jnp.bfloat16


def swap(value, axis):
    return lax.ppermute(value, axis, [(0, 1), (1, 0)])


def swap_both(value):
    return lax.ppermute(value, ("j", "x"), [(i, 3 - i) for i in range(4)])


def exchange(blocks, sign):
    count = lax.axis_size("e")
    if count <= 8:
        return [
            lax.ppermute(b, "e", [(i, (i + sign * s) % count) for i in range(count)])
            for s, b in enumerate(blocks)
            if s
        ]
    mine, order = lax.axis_index("e"), jnp.arange(count)
    to = jnp.take(jnp.stack(blocks), sign * (order - mine) % count, axis=0)
    came = lax.all_to_all(to, "e", 0, 0, tiled=True)
    came = jnp.take(came, (mine - sign * order) % count, axis=0)
    return [came[s] for s in range(1, count)]


def dot(a, b, ca, cb):
    return lax.dot_general(a, b, (((ca,), (cb,)), ((), ())), preferred_element_type=F32)


def prepare(experts, cap, quarter, index_ref, routes_ref, weights_ref, resid_ref, grad_ref, *outs):
    sends, sel_ref = outs[:-1], outs[-1]
    tokens = resid_ref.shape[0]
    mine, column = index_ref[0], index_ref[1]
    resid = resid_ref[...].astype(F32)
    inv_rms = lax.rsqrt(jnp.mean(resid * resid, axis=-1, keepdims=True) + epsilon)
    cols = pl.ds(pl.multiple_of(column * quarter, quarter), quarter)
    normed = (resid_ref[:, cols].astype(F32) * inv_rms).astype(BF16)
    grad = grad_ref[:, cols]
    first, second = routes_ref[0:1, :], routes_ref[1:2, :]
    first = jnp.where(first >= mine, first - mine, first - mine + experts)
    second = jnp.where(second >= mine, second - mine, second - mine + experts)
    ids = lax.broadcasted_iota(jnp.int32, (experts, tokens), 0)
    in_first, in_second = ids == first, ids == second
    member = jnp.where(in_first | in_second, 1.0, 0.0)
    before = jnp.where(
        lax.broadcasted_iota(jnp.int32, (tokens, tokens), 0)
        < lax.broadcasted_iota(jnp.int32, (tokens, tokens), 1),
        1.0,
        0.0,
    )
    rank = dot(member.astype(BF16), before.astype(BF16), 1, 0)
    rank_first = jnp.sum(jnp.where(in_first, rank, 0.0), axis=0, keepdims=True).astype(jnp.int32)
    rank_second = jnp.sum(jnp.where(in_second, rank, 0.0), axis=0, keepdims=True).astype(jnp.int32)
    slot_first = first * cap + rank_first
    slot_second = second * cap + rank_second
    for step in range(experts):
        slots = lax.broadcasted_iota(jnp.int32, (cap, tokens), 0) + step * cap
        hit_first, hit_second = slots == slot_first, slots == slot_second
        pick = jnp.where(hit_first | hit_second, 1.0, 0.0).astype(BF16)
        share = jnp.where(hit_first, weights_ref[0:1, :], 0.0) + jnp.where(
            hit_second, weights_ref[1:2, :], 0.0
        )
        share = jnp.sum(share, axis=1, keepdims=True)
        sel_ref[step] = pick
        sends[step][0] = dot(pick, normed, 1, 0).astype(BF16)
        sends[step][1] = (share * dot(pick, grad, 1, 0)).astype(BF16)


def columns(place, step, width):
    return pl.ds(pl.multiple_of((place ^ step) * width, width), width)


def first_half(
    cap,
    place_ref,
    own_ref,
    own_sib_ref,
    own_y_ref,
    own_y_sib_ref,
    pair_ref,
    pair_sib_ref,
    near_own_ref,
    near_own_sib_ref,
    near_ref,
    near_sib_ref,
    gate_ref,
    up_ref,
    down_ref,
    rows_ref,
    pre_gate_ref,
    pre_up_ref,
    near_out_ref,
    half_ref,
):
    place = place_ref[1]
    quarter = pair_ref.shape[-1]
    count = cap + pair_ref.shape[1]
    sides = (
        (own_ref, own_y_ref, pair_ref, near_own_ref, near_ref),
        (own_sib_ref, own_y_sib_ref, pair_sib_ref, near_own_sib_ref, near_sib_ref),
    )
    for dc, (own, own_y, pair, near_own, near) in enumerate(sides):
        for dx in range(2):
            cols = columns(place, 2 * dx + dc, quarter)
            rows_ref[:cap, cols] = own[dx * cap : (dx + 1) * cap]
            rows_ref[cap:count, cols] = pair[dx]
            rows_ref[count:, cols] = own_y[dx * cap : (dx + 1) * cap]
        cols = slice(dc * quarter, (dc + 1) * quarter)
        for dj in range(2):
            near_out_ref[dj * count : dj * count + cap, cols] = near_own[dj]
            near_out_ref[dj * count + cap : (dj + 1) * count, cols] = near[dj]
    rows = rows_ref[...]
    pre_gate_ref[...] = dot(rows, gate_ref[...], 1, 0)
    pre_up_ref[...] = dot(rows, up_ref[...], 1, 0)
    half_ref[...] = dot(
        near_out_ref[:, :quarter], down_ref[:, columns(place, 0, quarter)], 1, 1
    ) + dot(near_out_ref[:, quarter:], down_ref[:, columns(place, 1, quarter)], 1, 1)


def second_half(
    cap,
    place_ref,
    rows_y_ref,
    rows_y_sib_ref,
    far_own_ref,
    far_own_sib_ref,
    far_ref,
    far_sib_ref,
    pre_gate_ref,
    pre_up_ref,
    half_ref,
    gate_ref,
    up_ref,
    down_ref,
    rows_ref,
    far_out_ref,
    hidden_ref,
    d_gate_ref,
    d_up_ref,
    away_ref,
    late_gate_ref,
    late_up_ref,
):
    place = place_ref[1]
    quarter = far_ref.shape[-1]
    count = cap + far_ref.shape[1]
    early = pre_gate_ref.shape[0]
    sides = ((rows_y_ref, far_own_ref, far_ref), (rows_y_sib_ref, far_own_sib_ref, far_sib_ref))
    for dc, (rows_y, far_own, far) in enumerate(sides):
        for dx in range(2):
            rows_ref[:, columns(place, 2 * dx + dc, quarter)] = rows_y[dx]
        cols = slice(dc * quarter, (dc + 1) * quarter)
        for dj in range(2):
            far_out_ref[dj * count : dj * count + cap, cols] = far_own[dj]
            far_out_ref[dj * count + cap : (dj + 1) * count, cols] = far[dj]
    rows = rows_ref[...]
    late_gate_ref[...] = dot(rows, gate_ref[...], 1, 0)
    late_up_ref[...] = dot(rows, up_ref[...], 1, 0)
    for low, high, gate_at, up_at in (
        (0, early, pre_gate_ref, pre_up_ref),
        (early, 2 * count, late_gate_ref, late_up_ref),
    ):
        part = slice(low, high)
        d_hidden = half_ref[part] + (
            dot(far_out_ref[part, :quarter], down_ref[:, columns(place, 2, quarter)], 1, 1)
            + dot(far_out_ref[part, quarter:], down_ref[:, columns(place, 3, quarter)], 1, 1)
        )
        pre_gate, pre_up = gate_at[...], up_at[...]
        sigmoid_gate = jax.nn.sigmoid(pre_gate)
        activated = pre_gate * sigmoid_gate
        hidden_ref[part] = (activated * pre_up).astype(BF16)
        d_gate_ref[part] = (
            d_hidden * pre_up * sigmoid_gate * (1.0 + pre_gate * (1.0 - sigmoid_gate))
        ).astype(BF16)
        d_up_ref[part] = (d_hidden * activated).astype(BF16)
    for dx in range(2):
        block = columns(place, 2 * dx + 1, quarter)
        away_ref[:, dx * quarter : (dx + 1) * quarter] = (
            dot(d_gate_ref[...], gate_ref[block], 1, 1) + dot(d_up_ref[...], up_ref[block], 1, 1)
        ).astype(BF16)


def kept_part(place_ref, d_gate_ref, d_up_ref, gate_ref, up_ref, kept_ref):
    place = place_ref[1]
    quarter = kept_ref.shape[1] // 2
    for dx in range(2):
        block = columns(place, 2 * dx, quarter)
        kept_ref[:, dx * quarter : (dx + 1) * quarter] = dot(
            d_gate_ref[...], gate_ref[block], 1, 1
        ) + dot(d_up_ref[...], up_ref[block], 1, 1)


def join(place_ref, kept_ref, other_ref, *block_refs):
    count, quarter = block_refs[0].shape
    for i, block_ref in enumerate(block_refs):
        rows, cols = divmod(i, 2)
        rows = slice(rows * count, (rows + 1) * count)
        cols = slice(cols * quarter, (cols + 1) * quarter)
        block_ref[...] = (kept_ref[rows, cols] + other_ref[rows, cols].astype(F32)).astype(BF16)


def weight_grads(
    place_ref, early_ref, late_ref, near_ref, far_ref, hidden_ref, d_up_ref, up_ref, down_ref
):
    place = place_ref[1]
    early, features = early_ref.shape
    quarter = features // 4
    for dx, grads in enumerate((near_ref, far_ref)):
        for dc in range(2):
            down_ref[0, :, columns(place, 2 * dx + dc, quarter)] = dot(
                hidden_ref[...], grads[:, dc * quarter : (dc + 1) * quarter], 0, 0
            ).astype(BF16)
    for q in range(4):
        cols = slice(q * quarter, (q + 1) * quarter)
        up_ref[0, cols, :] = (
            dot(early_ref[:, cols], d_up_ref[:early], 0, 0)
            + dot(late_ref[:, cols], d_up_ref[early:], 0, 0)
        ).astype(BF16)


def order_mixed(index_ref, *refs):
    came, outs = refs[:-2], refs[-2:]
    experts = len(came)
    mine, half, core = index_ref[0], index_ref[2], index_ref[3]
    _, part, quarter = came[0].shape
    channels = quarter // 2
    for s in range(experts):
        source = jnp.where(mine >= s, mine - s, mine - s + experts)
        for dj in range(2):
            rows = pl.ds(pl.multiple_of((source * 2 + (half ^ dj)) * part, part), part)
            for d in range(2):
                lanes = pl.ds(pl.multiple_of((core ^ d) * channels, channels), channels)
                outs[d][rows] = came[s][dj, :, lanes]


def finish(core_ref, d_normed_ref, resid_ref, grad_ref, out_ref, blocks_ref):
    d_normed = d_normed_ref[...].astype(F32)
    resid = resid_ref[...].astype(F32)
    inv_rms = lax.rsqrt(jnp.mean(resid * resid, axis=-1, keepdims=True) + epsilon)
    unit = resid * inv_rms
    row_mean = jnp.mean(unit * d_normed, axis=-1, keepdims=True)
    out_ref[...] = (
        grad_ref[...].astype(F32) + inv_rms * (d_normed - unit * row_mean)
    ).astype(BF16)
    count, part, width = blocks_ref.shape
    mine = pl.ds(pl.multiple_of(core_ref[3] * part, part), part)
    for s in range(count):
        blocks_ref[s] = out_ref[mine, s * width : (s + 1) * width]


def in_vmem(kernel, outs, scratch, flops, limit, scalars, *values):
    vmem = pl.BlockSpec(memory_space=pltpu.VMEM)
    return pl.pallas_call(
        kernel,
        out_shape=[jax.ShapeDtypeStruct(shape, kind) for shape, kind in outs],
        in_specs=[pl.BlockSpec(memory_space=pltpu.SMEM)] + [vmem] * len(values),
        out_specs=[vmem] * len(outs),
        scratch_shapes=scratch,
        cost_estimate=pl.CostEstimate(flops=flops, bytes_accessed=0, transcendentals=0),
        compiler_params=pltpu.CompilerParams(vmem_limit_bytes=limit),
    )(scalars, *values)


def per_device(
    out_grad,
    residual,
    routes,
    route_weights,
    w_gate,
    w_up,
    w_down,
    out_gate,
    in_gate,
    conv_input,
    conv_out,
    conv_taps,
    w_out,
):
    tokens, features = out_grad.shape
    experts = lax.axis_size("e")
    slices = 2 * experts
    cap = -(-(5 * tokens // slices) // 16) * 16
    quarter = features // 4
    mine, half, core = lax.axis_index("e"), lax.axis_index("j"), lax.axis_index("c")
    place = 2 * lax.axis_index("x") + core
    index = jnp.stack([mine, place, half, core]).astype(jnp.int32)

    outs = in_vmem(
        functools.partial(prepare, experts, cap, quarter),
        [((2, cap, quarter), BF16)] * experts + [((experts, cap, tokens), BF16)],
        [],
        4 * experts * cap * tokens * quarter,
        60 * 2**20,
        index,
        routes.T,
        route_weights.T,
        residual,
        out_grad,
    )
    sends, sel = outs[:-1], outs[-1]
    conv_f32 = conv_out.astype(F32)
    gate_f32 = out_gate.astype(F32)
    mixed = (gate_f32 * conv_f32).astype(BF16)
    channels = mixed.shape[1]
    part = tokens // 2
    assert 2 * channels == quarter
    mixed_wide = jnp.concatenate([mixed[:part], mixed[part:]], axis=1)

    came = exchange(sends, 1)
    own_rows, own_grads = sends[0][0], sends[0][1]
    own_rows_x, own_grads_y = lax.optimization_barrier((swap(own_rows, "x"), swap(own_grads, "j")))
    own_pair = jnp.concatenate([own_rows, own_rows_x, mixed_wide], axis=0)
    own_near = jnp.stack([own_grads, own_grads_y])
    own_y = swap(own_pair, "j")
    own_far = swap(own_near, "x")
    came = lax.optimization_barrier(came)
    rows_z = jnp.concatenate([b[0] for b in came], axis=0)
    grads_z = jnp.concatenate([b[1] for b in came], axis=0)
    count = experts * cap

    rows_x, grads_y, own_y, own_far = lax.optimization_barrier(
        (swap(rows_z, "x"), swap(grads_z, "j"), own_y, own_far)
    )
    pair = jnp.stack([rows_z, rows_x])
    near = jnp.stack([grads_z, grads_y])
    own_far_sib = swap(own_far, "c")
    rows_y, far, own_far_sib = lax.optimization_barrier(
        (swap(pair, "j"), swap(near, "x"), own_far_sib)
    )
    weights = (w_gate[0], w_up[0], w_down[0])
    hidden_units = weights[0].shape[1]
    early = count + cap
    grant = 7 * 4 * 2 * count * hidden_units
    sib = lambda value: (value, swap(value, "c"))
    rows_early, pre_gate, pre_up, grads_near, d_half = in_vmem(
        functools.partial(first_half, cap),
        [
            ((early, features), BF16),
            ((early, hidden_units), F32),
            ((early, hidden_units), F32),
            ((2 * count, features // 2), BF16),
            ((2 * count, hidden_units), F32),
        ],
        [],
        (4 * early + 2 * count) * features * hidden_units,
        grant,
        index,
        *sib(own_pair),
        *sib(own_y),
        *sib(pair),
        *sib(own_near),
        *sib(near),
        *weights,
    )
    rows_late, grads_far, hidden, d_gate, d_up, away = in_vmem(
        functools.partial(second_half, cap),
        [
            ((2 * count - early, features), BF16),
            ((2 * count, features // 2), BF16),
            ((2 * count, hidden_units), BF16),
            ((2 * count, hidden_units), BF16),
            ((2 * count, hidden_units), BF16),
            ((2 * count, features // 2), BF16),
        ],
        [pltpu.VMEM((2 * count - early, hidden_units), F32)] * 2,
        (4 * (2 * count - early) + 6 * count) * features * hidden_units,
        grant,
        index,
        *sib(rows_y),
        own_far,
        own_far_sib,
        *sib(far),
        pre_gate,
        pre_up,
        d_half,
        *weights,
    )

    other = swap(away, "c")
    (kept,) = in_vmem(
        kept_part,
        [((2 * count, features // 2), F32)],
        [],
        4 * count * features * hidden_units,
        grant,
        index,
        d_gate,
        d_up,
        *weights[:2],
    )
    blocks = in_vmem(
        join, [((count, quarter), BF16)] * 4, [], 2 * count * features, grant, index, kept, other
    )
    mixed_mine = jnp.stack([own_pair[2 * cap :], own_y[2 * cap :]])
    mixed_rel = [mixed_mine] + exchange([mixed_mine] * experts, 1)
    summed = (
        blocks[0].astype(F32)
        + swap(blocks[1], "x").astype(F32)
        + swap(blocks[2], "j").astype(F32)
        + swap_both(blocks[3]).astype(F32)
    ).astype(BF16)
    summed, mixed_rel = lax.optimization_barrier((summed, mixed_rel))
    back = [summed[s * cap : (s + 1) * cap] for s in range(experts)]
    back = back[:1] + exchange(back, -1)

    grad_up, grad_down = in_vmem(
        weight_grads,
        [((1, features, hidden_units), BF16), ((1, hidden_units, features), BF16)],
        [],
        8 * count * features * hidden_units,
        3 * grant,
        index,
        rows_early,
        rows_late,
        grads_near,
        grads_far,
        hidden,
        d_up,
    )

    d_part = dot(
        sel.reshape(experts * cap, tokens), jnp.concatenate(back, axis=0), 0, 0
    ).astype(BF16)
    d_normed = lax.all_gather(d_part, ("x", "c"), axis=1, tiled=True)
    width = features // slices
    cut = slices if width % 128 == 0 else 1
    grad_resid, blocks = in_vmem(
        finish,
        [((tokens, features), BF16), ((cut, part, features // cut), BF16)],
        [],
        16 * tokens * features,
        8 * 2**20,
        index,
        d_normed,
        residual,
        out_grad,
    )

    ordered = in_vmem(
        order_mixed,
        [((slices * part, channels), BF16)] * 2,
        [],
        2 * slices * part * channels,
        grant,
        index,
        *mixed_rel,
    )
    if cut == 1:
        blocks = jnp.transpose(blocks.reshape(part, slices, width), (1, 0, 2))
    got = lax.all_to_all(blocks, ("e", "j"), 0, 0, tiled=True).reshape(slices * part, width)
    got_sib = swap(got, "c")
    grad_w_out = dot(got, ordered[0], 0, 0)
    grad_w_out = grad_w_out + dot(got_sib, ordered[1], 0, 0)

    d_mix = dot(grad_resid, w_out, 1, 1)
    grad_out_gate = (d_mix * conv_f32).astype(BF16)
    d_conv = d_mix * gate_f32
    edge = d_conv.astype(BF16)
    ends = slices - 1
    above = lax.ppermute(edge[-1:], ("e", "j"), [(i, i + 1) for i in range(ends)])
    below = lax.ppermute(edge[:1], ("e", "j"), [(i + 1, i) for i in range(ends)])
    above, below = above.astype(F32), below.astype(F32)
    later = jnp.concatenate([d_conv[1:], below], axis=0)
    earlier = jnp.concatenate([above, d_conv[:-1]], axis=0)
    d_inner = conv_taps[0] * later + conv_taps[1] * d_conv + conv_taps[2] * earlier
    grad_in_gate = (d_inner * conv_input.astype(F32)).astype(BF16)
    grad_conv_input = (d_inner * in_gate.astype(F32)).astype(BF16)
    return (
        grad_resid,
        grad_up,
        grad_down,
        grad_out_gate,
        grad_in_gate,
        grad_conv_input,
        grad_w_out,
    )


def solution(mesh):
    slices, blocks = mesh.shape["sp"], mesh.shape["tp"]
    grid = mesh.devices.reshape(slices // 2, 2, blocks // 2, 2)
    inner = Mesh(grid, ("e", "j", "x", "c"))
    sp, tp = ("e", "j"), ("x", "c")
    in_specs = (
        P(sp, None),
        P(sp, None),
        P(sp, None),
        P(sp, None),
        P(sp, None, tp),
        P(sp, None, tp),
        P(sp, tp, None),
        P(sp, tp),
        P(sp, tp),
        P(sp, tp),
        P(sp, tp),
        P(None, tp),
        P(tp, None),
    )
    out_specs = (
        P(sp, None),
        P(sp, None, tp),
        P(sp, tp, None),
        P(sp, tp),
        P(sp, tp),
        P(sp, tp),
        P(sp, tp),
    )

    return jax.shard_map(
        per_device, mesh=inner, in_specs=in_specs, out_specs=out_specs, check_vma=False
    )
```

```python
import functools

import jax
import jax.numpy as jnp
from jax import lax
from jax.experimental import pallas as pl
from jax.experimental.pallas import tpu as pltpu
from jax.sharding import Mesh
from jax.sharding import PartitionSpec as P


epsilon = 1e-06
F32 = jnp.float32
BF16 = jnp.bfloat16


def swap(value, axis):
    return lax.ppermute(value, axis, [(0, 1), (1, 0)])


def swap_both(value):
    return lax.ppermute(value, ("j", "x"), [(i, 3 - i) for i in range(4)])


def exchange(blocks, sign):
    count = lax.axis_size("e")
    if count <= 8:
        came = []
        for s, b in enumerate(blocks, 1):
            came.append(lax.ppermute(b, "e", [(i, (i + sign * s) % count) for i in range(count)]))
        return came
    mine, order = lax.axis_index("e"), jnp.arange(count)
    to = jnp.take(jnp.stack([blocks[0], *blocks]), sign * (order - mine) % count, axis=0)
    came = lax.all_to_all(to, "e", 0, 0, tiled=True)
    came = jnp.take(came, (mine - sign * order) % count, axis=0)
    return [came[s] for s in range(1, count)]


def dot(a, b, ca, cb):
    return lax.dot_general(a, b, (((ca,), (cb,)), ((), ())), preferred_element_type=F32)


def prepare(experts, cap, quarter, index_ref, routes_ref, weights_ref, resid_ref, grad_ref, *outs):
    sel_ref = outs[-1]
    sends = ((outs[0], outs[1]), *[(send.at[0], send.at[1]) for send in outs[2:-1]])
    tokens = resid_ref.shape[0]
    mine, column = index_ref[0], index_ref[1]
    resid = resid_ref[...].astype(F32)
    inv_rms = lax.rsqrt(jnp.mean(resid * resid, axis=-1, keepdims=True) + epsilon)
    cols = pl.ds(pl.multiple_of(column * quarter, quarter), quarter)
    normed = (resid_ref[:, cols].astype(F32) * inv_rms).astype(BF16)
    grad = grad_ref[:, cols]
    first, second = routes_ref[0:1, :], routes_ref[1:2, :]
    first = jnp.where(first >= mine, first - mine, first - mine + experts)
    second = jnp.where(second >= mine, second - mine, second - mine + experts)
    ids = lax.broadcasted_iota(jnp.int32, (experts, tokens), 0)
    in_first, in_second = ids == first, ids == second
    member = jnp.where(in_first | in_second, 1.0, 0.0)
    before = jnp.where(
        lax.broadcasted_iota(jnp.int32, (tokens, tokens), 0)
        < lax.broadcasted_iota(jnp.int32, (tokens, tokens), 1),
        1.0,
        0.0,
    )
    rank = dot(member.astype(BF16), before.astype(BF16), 1, 0)
    rank_first = jnp.sum(jnp.where(in_first, rank, 0.0), axis=0, keepdims=True).astype(jnp.int32)
    rank_second = jnp.sum(jnp.where(in_second, rank, 0.0), axis=0, keepdims=True).astype(jnp.int32)
    slot_first = first * cap + rank_first
    slot_second = second * cap + rank_second
    for step in range(experts):
        slots = lax.broadcasted_iota(jnp.int32, (cap, tokens), 0) + step * cap
        hit_first, hit_second = slots == slot_first, slots == slot_second
        pick = jnp.where(hit_first | hit_second, 1.0, 0.0).astype(BF16)
        share = jnp.where(hit_first, weights_ref[0:1, :], 0.0) + jnp.where(
            hit_second, weights_ref[1:2, :], 0.0
        )
        share = jnp.sum(share, axis=1, keepdims=True)
        sel_ref[step] = pick
        rows_ref, grads_ref = sends[step]
        rows_ref[...] = dot(pick, normed, 1, 0).astype(BF16)
        grads_ref[...] = (share * dot(pick, grad, 1, 0)).astype(BF16)


def columns(place, step, width):
    return pl.ds(pl.multiple_of((place ^ step) * width, width), width)


def activation(rows, gate_ref, up_ref, slope_ref, active_ref, hidden_ref):
    pre_gate = dot(rows, gate_ref[...], 1, 0)
    pre_up = dot(rows, up_ref[...], 1, 0)
    sigmoid_gate = jax.nn.sigmoid(pre_gate)
    activated = pre_gate * sigmoid_gate
    slope_ref[...] = pre_up * sigmoid_gate * (1.0 + pre_gate * (1.0 - sigmoid_gate))
    active_ref[...] = activated
    hidden_ref[...] = (activated * pre_up).astype(BF16)


def first_half(
    cap,
    place_ref,
    own_ref,
    own_sib_ref,
    own_y_ref,
    own_y_sib_ref,
    pair_ref,
    pair_sib_ref,
    near_own_ref,
    near_own_sib_ref,
    near_ref,
    near_sib_ref,
    gate_ref,
    up_ref,
    down_ref,
    rows_ref,
    slope_ref,
    active_ref,
    hidden_ref,
    near_out_ref,
    half_ref,
):
    place = place_ref[1]
    quarter = pair_ref.shape[-1]
    count = cap + pair_ref.shape[1]
    sides = (
        (own_ref, own_y_ref, pair_ref, near_own_ref, near_ref),
        (own_sib_ref, own_y_sib_ref, pair_sib_ref, near_own_sib_ref, near_sib_ref),
    )
    for dc, (own, own_y, pair, near_own, near) in enumerate(sides):
        for dx in range(2):
            cols = columns(place, 2 * dx + dc, quarter)
            rows_ref[:cap, cols] = own[dx * cap : (dx + 1) * cap]
            rows_ref[cap:count, cols] = pair[dx]
            rows_ref[count:, cols] = own_y[dx * cap : (dx + 1) * cap]
        cols = slice(dc * quarter, (dc + 1) * quarter)
        for dj in range(2):
            near_out_ref[dj * count : dj * count + cap, cols] = near_own[dj]
            near_out_ref[dj * count + cap : (dj + 1) * count, cols] = near[dj]
    activation(rows_ref[...], gate_ref, up_ref, slope_ref, active_ref, hidden_ref)
    half_ref[...] = dot(
        near_out_ref[:, :quarter], down_ref[:, columns(place, 0, quarter)], 1, 1
    ) + dot(near_out_ref[:, quarter:], down_ref[:, columns(place, 1, quarter)], 1, 1)


def second_half(
    cap,
    place_ref,
    rows_y_ref,
    rows_y_sib_ref,
    far_own_ref,
    far_own_sib_ref,
    far_ref,
    far_sib_ref,
    slope_ref,
    active_ref,
    half_ref,
    gate_ref,
    up_ref,
    down_ref,
    rows_ref,
    far_out_ref,
    hidden_ref,
    d_gate_ref,
    d_up_ref,
    away_ref,
    late_slope_ref,
    late_active_ref,
):
    place = place_ref[1]
    quarter = far_ref.shape[-1]
    count = cap + far_ref.shape[1]
    early = slope_ref.shape[0]
    sides = ((rows_y_ref, far_own_ref, far_ref), (rows_y_sib_ref, far_own_sib_ref, far_sib_ref))
    for dc, (rows_y, far_own, far) in enumerate(sides):
        for dx in range(2):
            rows_ref[:, columns(place, 2 * dx + dc, quarter)] = rows_y[dx]
        cols = slice(dc * quarter, (dc + 1) * quarter)
        for dj in range(2):
            far_out_ref[dj * count : dj * count + cap, cols] = far_own[dj]
            far_out_ref[dj * count + cap : (dj + 1) * count, cols] = far[dj]
    activation(rows_ref[...], gate_ref, up_ref, late_slope_ref, late_active_ref, hidden_ref)
    for low, high, slope, active in (
        (0, early, slope_ref, active_ref),
        (early, 2 * count, late_slope_ref, late_active_ref),
    ):
        part = slice(low, high)
        d_hidden = half_ref[part] + (
            dot(far_out_ref[part, :quarter], down_ref[:, columns(place, 2, quarter)], 1, 1)
            + dot(far_out_ref[part, quarter:], down_ref[:, columns(place, 3, quarter)], 1, 1)
        )
        d_gate_ref[part] = (d_hidden * slope[...]).astype(BF16)
        d_up_ref[part] = (d_hidden * active[...]).astype(BF16)
    for dx in range(2):
        block = columns(place, 2 * dx + 1, quarter)
        away_ref[:, dx * quarter : (dx + 1) * quarter] = (
            dot(d_gate_ref[...], gate_ref[block], 1, 1) + dot(d_up_ref[...], up_ref[block], 1, 1)
        ).astype(BF16)


def kept_part(place_ref, d_gate_ref, d_up_ref, gate_ref, up_ref, kept_ref):
    place = place_ref[1]
    quarter = kept_ref.shape[1] // 2
    for dx in range(2):
        block = columns(place, 2 * dx, quarter)
        kept_ref[:, dx * quarter : (dx + 1) * quarter] = dot(
            d_gate_ref[...], gate_ref[block], 1, 1
        ) + dot(d_up_ref[...], up_ref[block], 1, 1)


def join(place_ref, kept_ref, other_ref, *block_refs):
    cap, rest, quarter = block_refs[0].shape[0], block_refs[4].shape[0], block_refs[0].shape[1]
    for i in range(4):
        dj, dx = divmod(i, 2)
        cols = slice(dx * quarter, (dx + 1) * quarter)
        start = dj * (cap + rest)
        for block_ref, low, high in (
            (block_refs[i], start, start + cap),
            (block_refs[4 + i], start + cap, start + cap + rest),
        ):
            block_ref[...] = (
                kept_ref[low:high, cols] + other_ref[low:high, cols].astype(F32)
            ).astype(BF16)


def grad_of_down(place_ref, near_ref, far_ref, early_ref, late_ref, down_ref):
    place = place_ref[1]
    early = early_ref.shape[0]
    quarter = near_ref.shape[1] // 2
    for dx, grads in enumerate((near_ref, far_ref)):
        for dc in range(2):
            cols = slice(dc * quarter, (dc + 1) * quarter)
            down_ref[0, :, columns(place, 2 * dx + dc, quarter)] = (
                dot(early_ref[...], grads[:early, cols], 0, 0)
                + dot(late_ref[...], grads[early:, cols], 0, 0)
            ).astype(BF16)


def grad_of_up(place_ref, early_ref, late_ref, d_up_ref, up_ref):
    early, features = early_ref.shape
    quarter = features // 4
    for q in range(4):
        cols = slice(q * quarter, (q + 1) * quarter)
        up_ref[0, cols, :] = (
            dot(early_ref[:, cols], d_up_ref[:early], 0, 0)
            + dot(late_ref[:, cols], d_up_ref[early:], 0, 0)
        ).astype(BF16)


def order_mixed(index_ref, *refs):
    came, outs = refs[:-2], refs[-2:]
    experts = len(came)
    mine, half, core = index_ref[0], index_ref[2], index_ref[3]
    _, part, quarter = came[0].shape
    channels = quarter // 2
    for s in range(experts):
        source = jnp.where(mine >= s, mine - s, mine - s + experts)
        for dj in range(2):
            rows = pl.ds(pl.multiple_of((source * 2 + (half ^ dj)) * part, part), part)
            for d in range(2):
                lanes = pl.ds(pl.multiple_of((core ^ d) * channels, channels), channels)
                outs[d][rows] = came[s][dj, :, lanes]


def finish(
    core_ref,
    d_normed_ref,
    resid_ref,
    grad_ref,
    w_out_ref,
    conv_ref,
    gate_ref,
    out_ref,
    blocks_ref,
    out_gate_ref,
    d_conv_ref,
    first_ref,
    last_ref,
):
    d_normed = d_normed_ref[...].astype(F32)
    resid = resid_ref[...].astype(F32)
    inv_rms = lax.rsqrt(jnp.mean(resid * resid, axis=-1, keepdims=True) + epsilon)
    unit = resid * inv_rms
    row_mean = jnp.mean(unit * d_normed, axis=-1, keepdims=True)
    grad_resid = (
        grad_ref[...].astype(F32) + inv_rms * (d_normed - unit * row_mean)
    ).astype(BF16)
    out_ref[...] = grad_resid
    count, part, width = blocks_ref.shape
    mine = pl.ds(pl.multiple_of(core_ref[3] * part, part), part)
    for s in range(count):
        blocks_ref[s] = out_ref[mine, s * width : (s + 1) * width]
    d_mix = dot(grad_resid, w_out_ref[...], 1, 1)
    out_gate_ref[...] = (d_mix * conv_ref[...].astype(F32)).astype(BF16)
    d_conv = d_mix * gate_ref[...].astype(F32)
    d_conv_ref[...] = d_conv
    first_ref[...] = d_conv[:1].astype(BF16)
    last_ref[...] = d_conv[-1:].astype(BF16)


def in_vmem(kernel, outs, scratch, flops, limit, scalars, *values):
    vmem = pl.BlockSpec(memory_space=pltpu.VMEM)
    return pl.pallas_call(
        kernel,
        out_shape=[jax.ShapeDtypeStruct(shape, kind) for shape, kind in outs],
        in_specs=[pl.BlockSpec(memory_space=pltpu.SMEM)] + [vmem] * len(values),
        out_specs=[vmem] * len(outs),
        scratch_shapes=scratch,
        cost_estimate=pl.CostEstimate(flops=flops, bytes_accessed=0, transcendentals=0),
        compiler_params=pltpu.CompilerParams(vmem_limit_bytes=limit),
    )(scalars, *values)


def per_device(
    out_grad,
    residual,
    routes,
    route_weights,
    w_gate,
    w_up,
    w_down,
    out_gate,
    in_gate,
    conv_input,
    conv_out,
    conv_taps,
    w_out,
):
    tokens, features = out_grad.shape
    experts = lax.axis_size("e")
    slices = 2 * experts
    cap = -(-(5 * tokens // slices) // 16) * 16
    quarter = features // 4
    mine, half, core = lax.axis_index("e"), lax.axis_index("j"), lax.axis_index("c")
    place = 2 * lax.axis_index("x") + core
    index = jnp.stack([mine, place, half, core]).astype(jnp.int32)

    outs = in_vmem(
        functools.partial(prepare, experts, cap, quarter),
        [((cap, quarter), BF16)] * 2
        + [((2, cap, quarter), BF16)] * (experts - 1)
        + [((experts, cap, tokens), BF16)],
        [],
        4 * experts * cap * tokens * quarter,
        60 * 2**20,
        index,
        routes.T,
        route_weights.T,
        residual,
        out_grad,
    )
    own_rows, own_grads, sends, sel = outs[0], outs[1], outs[2:-1], outs[-1]
    conv_f32 = conv_out.astype(F32)
    gate_f32 = out_gate.astype(F32)
    mixed = (gate_f32 * conv_f32).astype(BF16)
    channels = mixed.shape[1]
    part = tokens // 2
    assert 2 * channels == quarter
    mixed_wide = jnp.concatenate([mixed[:part], mixed[part:]], axis=1)

    came = exchange(sends, 1)
    own_rows_x, own_grads_y = lax.optimization_barrier((swap(own_rows, "x"), swap(own_grads, "j")))
    own_pair = jnp.concatenate([own_rows, own_rows_x, mixed_wide], axis=0)
    own_near = jnp.stack([own_grads, own_grads_y])
    own_y = swap(own_pair, "j")
    own_far = swap(own_near, "x")
    came = lax.optimization_barrier(came)
    rows_z = jnp.concatenate([b[0] for b in came], axis=0)
    grads_z = jnp.concatenate([b[1] for b in came], axis=0)
    count = experts * cap

    rows_x, grads_y, own_y, own_far = lax.optimization_barrier(
        (swap(rows_z, "x"), swap(grads_z, "j"), own_y, own_far)
    )
    pair = jnp.stack([rows_z, rows_x])
    near = jnp.stack([grads_z, grads_y])
    own_far_sib = swap(own_far, "c")
    rows_y, far, own_far_sib = lax.optimization_barrier(
        (swap(pair, "j"), swap(near, "x"), own_far_sib)
    )
    weights = (w_gate[0], w_up[0], w_down[0])
    hidden_units = weights[0].shape[1]
    early = count + cap
    grant = 7 * 4 * 2 * count * hidden_units
    sib = lambda value: (value, swap(value, "c"))
    rows_early, slope, active, hidden_early, grads_near, d_half = in_vmem(
        functools.partial(first_half, cap),
        [
            ((early, features), BF16),
            ((early, hidden_units), F32),
            ((early, hidden_units), F32),
            ((early, hidden_units), BF16),
            ((2 * count, features // 2), BF16),
            ((2 * count, hidden_units), F32),
        ],
        [],
        (4 * early + 2 * count) * features * hidden_units,
        grant,
        index,
        *sib(own_pair),
        *sib(own_y),
        *sib(pair),
        *sib(own_near),
        *sib(near),
        *weights,
    )
    rows_late, grads_far, hidden_late, d_gate, d_up, away = in_vmem(
        functools.partial(second_half, cap),
        [
            ((2 * count - early, features), BF16),
            ((2 * count, features // 2), BF16),
            ((2 * count - early, hidden_units), BF16),
            ((2 * count, hidden_units), BF16),
            ((2 * count, hidden_units), BF16),
            ((2 * count, features // 2), BF16),
        ],
        [pltpu.VMEM((2 * count - early, hidden_units), F32)] * 2,
        (4 * (2 * count - early) + 6 * count) * features * hidden_units,
        grant,
        index,
        *sib(rows_y),
        own_far,
        own_far_sib,
        *sib(far),
        slope,
        active,
        d_half,
        *weights,
    )

    other = swap(away, "c")
    (kept,) = in_vmem(
        kept_part,
        [((2 * count, features // 2), F32)],
        [],
        4 * count * features * hidden_units,
        grant,
        index,
        d_gate,
        d_up,
        *weights[:2],
    )
    blocks = in_vmem(
        join,
        [((cap, quarter), BF16)] * 4 + [((count - cap, quarter), BF16)] * 4,
        [],
        2 * count * features,
        grant,
        index,
        kept,
        other,
    )
    mixed_mine = jnp.stack([own_pair[2 * cap :], own_y[2 * cap :]])
    mixed_rel = [mixed_mine] + exchange([mixed_mine] * (experts - 1), 1)

    def spread(parts):
        return [parts[0], swap(parts[1], "x"), swap(parts[2], "j"), swap_both(parts[3])]

    def total(parts):
        return sum(part.astype(F32) for part in parts).astype(BF16)

    own_layer = spread(blocks[:4])
    rest, mixed_rel = lax.optimization_barrier((total(spread(blocks[4:])), mixed_rel))
    back = exchange([rest[s * cap : (s + 1) * cap] for s in range(experts - 1)], -1)
    own_layer, back = lax.optimization_barrier((own_layer, back))
    back = [total(own_layer), *back]

    (grad_down,) = in_vmem(
        grad_of_down,
        [((1, hidden_units, features), BF16)],
        [],
        4 * count * features * hidden_units,
        2 * grant,
        index,
        grads_near,
        grads_far,
        hidden_early,
        hidden_late,
    )
    (grad_up,) = in_vmem(
        grad_of_up,
        [((1, features, hidden_units), BF16)],
        [],
        4 * count * features * hidden_units,
        2 * grant,
        index,
        rows_early,
        rows_late,
        d_up,
    )

    d_part = dot(
        sel.reshape(experts * cap, tokens), jnp.concatenate(back, axis=0), 0, 0
    ).astype(BF16)
    d_normed = lax.all_gather(d_part, ("x", "c"), axis=1, tiled=True)
    width = features // slices
    cut = slices if width % 128 == 0 else 1
    grad_resid, blocks, grad_out_gate, d_conv, first, last = in_vmem(
        finish,
        [
            ((tokens, features), BF16),
            ((cut, part, features // cut), BF16),
            ((tokens, channels), BF16),
            ((tokens, channels), F32),
            ((1, channels), BF16),
            ((1, channels), BF16),
        ],
        [],
        16 * tokens * features,
        8 * 2**20,
        index,
        d_normed,
        residual,
        out_grad,
        w_out,
        conv_out,
        out_gate,
    )

    ordered = in_vmem(
        order_mixed,
        [((slices * part, channels), BF16)] * 2,
        [],
        2 * slices * part * channels,
        grant,
        index,
        *mixed_rel,
    )
    if cut == 1:
        blocks = jnp.transpose(blocks.reshape(part, slices, width), (1, 0, 2))
    got = lax.all_to_all(blocks, ("e", "j"), 0, 0, tiled=True).reshape(slices * part, width)
    got_sib = swap(got, "c")
    grad_w_out = dot(got, ordered[0], 0, 0)
    grad_w_out = grad_w_out + dot(got_sib, ordered[1], 0, 0)

    ends = slices - 1
    above = lax.ppermute(last, ("e", "j"), [(i, i + 1) for i in range(ends)])
    below = lax.ppermute(first, ("e", "j"), [(i + 1, i) for i in range(ends)])
    above, below = above.astype(F32), below.astype(F32)
    later = jnp.concatenate([d_conv[1:], below], axis=0)
    earlier = jnp.concatenate([above, d_conv[:-1]], axis=0)
    d_inner = conv_taps[0] * later + conv_taps[1] * d_conv + conv_taps[2] * earlier
    grad_in_gate = (d_inner * conv_input.astype(F32)).astype(BF16)
    grad_conv_input = (d_inner * in_gate.astype(F32)).astype(BF16)
    return (
        grad_resid,
        grad_up,
        grad_down,
        grad_out_gate,
        grad_in_gate,
        grad_conv_input,
        grad_w_out,
    )


def solution(mesh):
    slices, blocks = mesh.shape["sp"], mesh.shape["tp"]
    grid = mesh.devices.reshape(slices // 2, 2, blocks // 2, 2)
    inner = Mesh(grid, ("e", "j", "x", "c"))
    sp, tp = ("e", "j"), ("x", "c")
    in_specs = (
        P(sp, None),
        P(sp, None),
        P(sp, None),
        P(sp, None),
        P(sp, None, tp),
        P(sp, None, tp),
        P(sp, tp, None),
        P(sp, tp),
        P(sp, tp),
        P(sp, tp),
        P(sp, tp),
        P(None, tp),
        P(tp, None),
    )
    out_specs = (
        P(sp, None),
        P(sp, None, tp),
        P(sp, tp, None),
        P(sp, tp),
        P(sp, tp),
        P(sp, tp),
        P(sp, tp),
    )

    return jax.shard_map(
        per_device, mesh=inner, in_specs=in_specs, out_specs=out_specs, check_vma=False
    )
```

```python
import functools

import jax
import jax.numpy as jnp
from jax import lax
from jax.experimental import pallas as pl
from jax.experimental.pallas import tpu as pltpu
from jax.sharding import Mesh
from jax.sharding import PartitionSpec as P


epsilon = 1e-06
F32 = jnp.float32
BF16 = jnp.bfloat16


def swap(value, axis):
    return lax.ppermute(value, axis, [(0, 1), (1, 0)])


def swap_both(value):
    return lax.ppermute(value, ("j", "x"), [(i, 3 - i) for i in range(4)])


def exchange(blocks, sign):
    count = lax.axis_size("e")
    if count <= 8:
        came = []
        for s, b in enumerate(blocks, 1):
            came.append(lax.ppermute(b, "e", [(i, (i + sign * s) % count) for i in range(count)]))
        return came
    mine, order = lax.axis_index("e"), jnp.arange(count)
    to = jnp.take(jnp.stack([blocks[0], *blocks]), sign * (order - mine) % count, axis=0)
    came = lax.all_to_all(to, "e", 0, 0, tiled=True)
    came = jnp.take(came, (mine - sign * order) % count, axis=0)
    return [came[s] for s in range(1, count)]


def dot(a, b, ca, cb):
    return lax.dot_general(a, b, (((ca,), (cb,)), ((), ())), preferred_element_type=F32)


def prepare(experts, cap, quarter, routes_ref, weights_ref, resid_ref, grad_ref, *outs):
    sel_ref = outs[-1]
    sends = ((outs[0], outs[1]), *[(send.at[0], send.at[1]) for send in outs[2:-1]])
    tokens = resid_ref.shape[0]
    mine, column = lax.axis_index("e"), 2 * lax.axis_index("x") + lax.axis_index("c")
    resid = resid_ref[...].astype(F32)
    inv_rms = lax.rsqrt(jnp.mean(resid * resid, axis=-1, keepdims=True) + epsilon)
    cols = pl.ds(pl.multiple_of(column * quarter, quarter), quarter)
    normed = (resid_ref[:, cols].astype(F32) * inv_rms).astype(BF16)
    grad = grad_ref[:, cols]
    first, second = routes_ref[0:1, :], routes_ref[1:2, :]
    first = jnp.where(first >= mine, first - mine, first - mine + experts)
    second = jnp.where(second >= mine, second - mine, second - mine + experts)
    ids = lax.broadcasted_iota(jnp.int32, (experts, tokens), 0)
    in_first, in_second = ids == first, ids == second
    member = jnp.where(in_first | in_second, 1.0, 0.0)
    before = jnp.where(
        lax.broadcasted_iota(jnp.int32, (tokens, tokens), 0)
        < lax.broadcasted_iota(jnp.int32, (tokens, tokens), 1),
        1.0,
        0.0,
    )
    rank = dot(member.astype(BF16), before.astype(BF16), 1, 0)
    rank_first = jnp.sum(jnp.where(in_first, rank, 0.0), axis=0, keepdims=True).astype(jnp.int32)
    rank_second = jnp.sum(jnp.where(in_second, rank, 0.0), axis=0, keepdims=True).astype(jnp.int32)
    slot_first = first * cap + rank_first
    slot_second = second * cap + rank_second
    for step in range(experts):
        slots = lax.broadcasted_iota(jnp.int32, (cap, tokens), 0) + step * cap
        hit_first, hit_second = slots == slot_first, slots == slot_second
        pick = jnp.where(hit_first | hit_second, 1.0, 0.0).astype(BF16)
        share = jnp.where(hit_first, weights_ref[0:1, :], 0.0) + jnp.where(
            hit_second, weights_ref[1:2, :], 0.0
        )
        share = jnp.sum(share, axis=1, keepdims=True)
        sel_ref[step] = pick
        rows_ref, grads_ref = sends[step]
        rows_ref[...] = dot(pick, normed, 1, 0).astype(BF16)
        grads_ref[...] = (share * dot(pick, grad, 1, 0)).astype(BF16)


def columns(place, step, width):
    return pl.ds(pl.multiple_of((place ^ step) * width, width), width)


def activation(rows, gate_ref, up_ref, slope_ref, active_ref, hidden_ref):
    pre_gate = dot(rows, gate_ref[...], 1, 0)
    pre_up = dot(rows, up_ref[...], 1, 0)
    sigmoid_gate = jax.nn.sigmoid(pre_gate)
    activated = pre_gate * sigmoid_gate
    slope_ref[...] = pre_up * sigmoid_gate * (1.0 + pre_gate * (1.0 - sigmoid_gate))
    active_ref[...] = activated
    hidden_ref[...] = (activated * pre_up).astype(BF16)


def first_half(
    cap,
    own_ref,
    own_sib_ref,
    own_y_ref,
    own_y_sib_ref,
    pair_ref,
    pair_sib_ref,
    near_own_ref,
    near_own_sib_ref,
    near_ref,
    near_sib_ref,
    gate_ref,
    up_ref,
    down_ref,
    rows_ref,
    slope_ref,
    active_ref,
    hidden_ref,
    near_out_ref,
    half_ref,
):
    place = 2 * lax.axis_index("x") + lax.axis_index("c")
    quarter = pair_ref.shape[-1]
    count = cap + pair_ref.shape[1]
    sides = (
        (own_ref, own_y_ref, pair_ref, near_own_ref, near_ref),
        (own_sib_ref, own_y_sib_ref, pair_sib_ref, near_own_sib_ref, near_sib_ref),
    )
    for dc, (own, own_y, pair, near_own, near) in enumerate(sides):
        for dx in range(2):
            cols = columns(place, 2 * dx + dc, quarter)
            rows_ref[:cap, cols] = own[dx * cap : (dx + 1) * cap]
            rows_ref[cap:count, cols] = pair[dx]
            rows_ref[count:, cols] = own_y[dx * cap : (dx + 1) * cap]
        cols = slice(dc * quarter, (dc + 1) * quarter)
        for dj in range(2):
            near_out_ref[dj * count : dj * count + cap, cols] = near_own[dj]
            near_out_ref[dj * count + cap : (dj + 1) * count, cols] = near[dj]
    activation(rows_ref[...], gate_ref, up_ref, slope_ref, active_ref, hidden_ref)
    half_ref[...] = dot(
        near_out_ref[:, :quarter], down_ref[:, columns(place, 0, quarter)], 1, 1
    ) + dot(near_out_ref[:, quarter:], down_ref[:, columns(place, 1, quarter)], 1, 1)


def second_half(
    cap,
    rows_y_ref,
    rows_y_sib_ref,
    far_own_ref,
    far_own_sib_ref,
    far_ref,
    far_sib_ref,
    slope_ref,
    active_ref,
    half_ref,
    gate_ref,
    up_ref,
    down_ref,
    rows_ref,
    far_out_ref,
    hidden_ref,
    d_gate_ref,
    d_up_ref,
    away_ref,
    late_slope_ref,
    late_active_ref,
):
    place = 2 * lax.axis_index("x") + lax.axis_index("c")
    quarter = far_ref.shape[-1]
    count = cap + far_ref.shape[1]
    early = slope_ref.shape[0]
    sides = ((rows_y_ref, far_own_ref, far_ref), (rows_y_sib_ref, far_own_sib_ref, far_sib_ref))
    for dc, (rows_y, far_own, far) in enumerate(sides):
        for dx in range(2):
            rows_ref[:, columns(place, 2 * dx + dc, quarter)] = rows_y[dx]
        cols = slice(dc * quarter, (dc + 1) * quarter)
        for dj in range(2):
            far_out_ref[dj * count : dj * count + cap, cols] = far_own[dj]
            far_out_ref[dj * count + cap : (dj + 1) * count, cols] = far[dj]
    activation(rows_ref[...], gate_ref, up_ref, late_slope_ref, late_active_ref, hidden_ref)
    for low, high, slope, active in (
        (0, early, slope_ref, active_ref),
        (early, 2 * count, late_slope_ref, late_active_ref),
    ):
        part = slice(low, high)
        d_hidden = half_ref[part] + (
            dot(far_out_ref[part, :quarter], down_ref[:, columns(place, 2, quarter)], 1, 1)
            + dot(far_out_ref[part, quarter:], down_ref[:, columns(place, 3, quarter)], 1, 1)
        )
        d_gate_ref[part] = (d_hidden * slope[...]).astype(BF16)
        d_up_ref[part] = (d_hidden * active[...]).astype(BF16)
    for dx in range(2):
        block = columns(place, 2 * dx + 1, quarter)
        away_ref[:, dx * quarter : (dx + 1) * quarter] = (
            dot(d_gate_ref[...], gate_ref[block], 1, 1) + dot(d_up_ref[...], up_ref[block], 1, 1)
        ).astype(BF16)


def kept_part(d_gate_ref, d_up_ref, gate_ref, up_ref, kept_ref):
    place = 2 * lax.axis_index("x") + lax.axis_index("c")
    quarter = kept_ref.shape[1] // 2
    for dx in range(2):
        block = columns(place, 2 * dx, quarter)
        kept_ref[:, dx * quarter : (dx + 1) * quarter] = dot(
            d_gate_ref[...], gate_ref[block], 1, 1
        ) + dot(d_up_ref[...], up_ref[block], 1, 1)


def join(kept_ref, other_ref, *block_refs):
    cap, rest, quarter = block_refs[0].shape[0], block_refs[4].shape[0], block_refs[0].shape[1]
    for i in range(4):
        dj, dx = divmod(i, 2)
        cols = slice(dx * quarter, (dx + 1) * quarter)
        start = dj * (cap + rest)
        for block_ref, low, high in (
            (block_refs[i], start, start + cap),
            (block_refs[4 + i], start + cap, start + cap + rest),
        ):
            block_ref[...] = (
                kept_ref[low:high, cols] + other_ref[low:high, cols].astype(F32)
            ).astype(BF16)


def grad_of_down(near_ref, far_ref, early_ref, late_ref, down_ref):
    place = 2 * lax.axis_index("x") + lax.axis_index("c")
    early = early_ref.shape[0]
    quarter = near_ref.shape[1] // 2
    for dx, grads in enumerate((near_ref, far_ref)):
        for dc in range(2):
            cols = slice(dc * quarter, (dc + 1) * quarter)
            down_ref[0, :, columns(place, 2 * dx + dc, quarter)] = (
                dot(early_ref[...], grads[:early, cols], 0, 0)
                + dot(late_ref[...], grads[early:, cols], 0, 0)
            ).astype(BF16)


def grad_of_up(early_ref, late_ref, d_up_ref, up_ref):
    early, features = early_ref.shape
    quarter = features // 4
    for q in range(4):
        cols = slice(q * quarter, (q + 1) * quarter)
        up_ref[0, cols, :] = (
            dot(early_ref[:, cols], d_up_ref[:early], 0, 0)
            + dot(late_ref[:, cols], d_up_ref[early:], 0, 0)
        ).astype(BF16)


def order_mixed(*refs):
    came, outs = refs[:-2], refs[-2:]
    experts = len(came)
    mine, half, core = lax.axis_index("e"), lax.axis_index("j"), lax.axis_index("c")
    _, part, quarter = came[0].shape
    channels = quarter // 2
    for s in range(experts):
        source = jnp.where(mine >= s, mine - s, mine - s + experts)
        for dj in range(2):
            rows = pl.ds(pl.multiple_of((source * 2 + (half ^ dj)) * part, part), part)
            for d in range(2):
                lanes = pl.ds(pl.multiple_of((core ^ d) * channels, channels), channels)
                outs[d][rows] = came[s][dj, :, lanes]


def finish(
    d_normed_ref,
    resid_ref,
    grad_ref,
    w_out_ref,
    conv_ref,
    gate_ref,
    out_ref,
    blocks_ref,
    out_gate_ref,
    d_conv_ref,
    first_ref,
    last_ref,
):
    d_normed = d_normed_ref[...].astype(F32)
    resid = resid_ref[...].astype(F32)
    inv_rms = lax.rsqrt(jnp.mean(resid * resid, axis=-1, keepdims=True) + epsilon)
    unit = resid * inv_rms
    row_mean = jnp.mean(unit * d_normed, axis=-1, keepdims=True)
    grad_resid = (
        grad_ref[...].astype(F32) + inv_rms * (d_normed - unit * row_mean)
    ).astype(BF16)
    out_ref[...] = grad_resid
    count, part, width = blocks_ref.shape
    mine = pl.ds(pl.multiple_of(lax.axis_index("c") * part, part), part)
    for s in range(count):
        blocks_ref[s] = out_ref[mine, s * width : (s + 1) * width]
    d_mix = dot(grad_resid, w_out_ref[...], 1, 1)
    out_gate_ref[...] = (d_mix * conv_ref[...].astype(F32)).astype(BF16)
    d_conv = d_mix * gate_ref[...].astype(F32)
    d_conv_ref[...] = d_conv
    first_ref[...] = d_conv[:1].astype(BF16)
    last_ref[...] = d_conv[-1:].astype(BF16)


def in_vmem(kernel, outs, scratch, flops, limit, *values):
    vmem = pl.BlockSpec(memory_space=pltpu.VMEM)
    return pl.pallas_call(
        kernel,
        out_shape=[jax.ShapeDtypeStruct(shape, kind) for shape, kind in outs],
        in_specs=[vmem] * len(values),
        out_specs=[vmem] * len(outs),
        scratch_shapes=scratch,
        cost_estimate=pl.CostEstimate(flops=flops, bytes_accessed=0, transcendentals=0),
        compiler_params=pltpu.CompilerParams(vmem_limit_bytes=limit),
    )(*values)


def per_device(
    out_grad,
    residual,
    routes,
    route_weights,
    w_gate,
    w_up,
    w_down,
    out_gate,
    in_gate,
    conv_input,
    conv_out,
    conv_taps,
    w_out,
):
    tokens, features = out_grad.shape
    experts = lax.axis_size("e")
    slices = 2 * experts
    cap = -(-(5 * tokens // slices) // 16) * 16
    quarter = features // 4
    outs = in_vmem(
        functools.partial(prepare, experts, cap, quarter),
        [((cap, quarter), BF16)] * 2
        + [((2, cap, quarter), BF16)] * (experts - 1)
        + [((experts, cap, tokens), BF16)],
        [],
        4 * experts * cap * tokens * quarter,
        60 * 2**20,
        routes.T,
        route_weights.T,
        residual,
        out_grad,
    )
    own_rows, own_grads, sends, sel = outs[0], outs[1], outs[2:-1], outs[-1]
    conv_f32 = conv_out.astype(F32)
    gate_f32 = out_gate.astype(F32)
    mixed = (gate_f32 * conv_f32).astype(BF16)
    channels = mixed.shape[1]
    part = tokens // 2
    assert 2 * channels == quarter
    mixed_wide = jnp.concatenate([mixed[:part], mixed[part:]], axis=1)

    came = exchange(sends, 1)
    own_rows_x, own_grads_y = lax.optimization_barrier((swap(own_rows, "x"), swap(own_grads, "j")))
    own_pair = jnp.concatenate([own_rows, own_rows_x, mixed_wide], axis=0)
    own_near = jnp.stack([own_grads, own_grads_y])
    own_y = swap(own_pair, "j")
    own_far = swap(own_near, "x")
    came = lax.optimization_barrier(came)
    rows_z = jnp.concatenate([b[0] for b in came], axis=0)
    grads_z = jnp.concatenate([b[1] for b in came], axis=0)
    count = experts * cap

    mixed_mine = jnp.stack([own_pair[2 * cap :], own_y[2 * cap :]])
    mixed_rel = [mixed_mine] + exchange([mixed_mine] * (experts - 1), 1)
    rows_x, grads_y, own_far = lax.optimization_barrier(
        (swap(rows_z, "x"), swap(grads_z, "j"), own_far)
    )
    pair = jnp.stack([rows_z, rows_x])
    near = jnp.stack([grads_z, grads_y])
    own_far_sib = swap(own_far, "c")
    rows_y, far, own_far_sib = lax.optimization_barrier(
        (swap(pair, "j"), swap(near, "x"), own_far_sib)
    )
    weights = (w_gate[0], w_up[0], w_down[0])
    hidden_units = weights[0].shape[1]
    early = count + cap
    grant = 7 * 4 * 2 * count * hidden_units
    sib = lambda value: (value, swap(value, "c"))
    rows_early, slope, active, hidden_early, grads_near, d_half = in_vmem(
        functools.partial(first_half, cap),
        [
            ((early, features), BF16),
            ((early, hidden_units), F32),
            ((early, hidden_units), F32),
            ((early, hidden_units), BF16),
            ((2 * count, features // 2), BF16),
            ((2 * count, hidden_units), F32),
        ],
        [],
        (4 * early + 2 * count) * features * hidden_units,
        grant,
        *sib(own_pair),
        *sib(own_y),
        *sib(pair),
        *sib(own_near),
        *sib(near),
        *weights,
    )
    rows_late, grads_far, hidden_late, d_gate, d_up, away = in_vmem(
        functools.partial(second_half, cap),
        [
            ((2 * count - early, features), BF16),
            ((2 * count, features // 2), BF16),
            ((2 * count - early, hidden_units), BF16),
            ((2 * count, hidden_units), BF16),
            ((2 * count, hidden_units), BF16),
            ((2 * count, features // 2), BF16),
        ],
        [pltpu.VMEM((2 * count - early, hidden_units), F32)] * 2,
        (4 * (2 * count - early) + 6 * count) * features * hidden_units,
        grant,
        *sib(rows_y),
        own_far,
        own_far_sib,
        *sib(far),
        slope,
        active,
        d_half,
        *weights,
    )

    other = swap(away, "c")
    (kept,) = in_vmem(
        kept_part,
        [((2 * count, features // 2), F32)],
        [],
        4 * count * features * hidden_units,
        grant,
        d_gate,
        d_up,
        *weights[:2],
    )
    blocks = in_vmem(
        join,
        [((cap, quarter), BF16)] * 4 + [((count - cap, quarter), BF16)] * 4,
        [],
        2 * count * features,
        grant,
        kept,
        other,
    )

    def spread(parts):
        return [parts[0], swap(parts[1], "x"), swap(parts[2], "j"), swap_both(parts[3])]

    def total(parts):
        return sum(part.astype(F32) for part in parts).astype(BF16)

    own_layer = spread(blocks[:4])
    rest, mixed_rel = lax.optimization_barrier((total(spread(blocks[4:])), mixed_rel))
    back = exchange([rest[s * cap : (s + 1) * cap] for s in range(experts - 1)], -1)
    own_layer, back = lax.optimization_barrier((own_layer, back))
    back = [total(own_layer), *back]

    (grad_down,) = in_vmem(
        grad_of_down,
        [((1, hidden_units, features), BF16)],
        [],
        4 * count * features * hidden_units,
        2 * grant,
        grads_near,
        grads_far,
        hidden_early,
        hidden_late,
    )
    (grad_up,) = in_vmem(
        grad_of_up,
        [((1, features, hidden_units), BF16)],
        [],
        4 * count * features * hidden_units,
        2 * grant,
        rows_early,
        rows_late,
        d_up,
    )

    d_part = dot(
        sel.reshape(experts * cap, tokens), jnp.concatenate(back, axis=0), 0, 0
    ).astype(BF16)
    d_normed = lax.all_gather(d_part, ("x", "c"), axis=1, tiled=True)
    width = features // slices
    cut = slices if width % 128 == 0 else 1
    grad_resid, blocks, grad_out_gate, d_conv, first, last = in_vmem(
        finish,
        [
            ((tokens, features), BF16),
            ((cut, part, features // cut), BF16),
            ((tokens, channels), BF16),
            ((tokens, channels), F32),
            ((1, channels), BF16),
            ((1, channels), BF16),
        ],
        [],
        16 * tokens * features,
        8 * 2**20,
        d_normed,
        residual,
        out_grad,
        w_out,
        conv_out,
        out_gate,
    )

    ordered = in_vmem(
        order_mixed,
        [((slices * part, channels), BF16)] * 2,
        [],
        2 * slices * part * channels,
        grant,
        *mixed_rel,
    )
    if cut == 1:
        blocks = jnp.transpose(blocks.reshape(part, slices, width), (1, 0, 2))
    got = lax.all_to_all(blocks, ("e", "j"), 0, 0, tiled=True).reshape(slices * part, width)
    got_sib = swap(got, "c")
    grad_w_out = dot(got, ordered[0], 0, 0)
    grad_w_out = grad_w_out + dot(got_sib, ordered[1], 0, 0)

    ends = slices - 1
    above = lax.ppermute(last, ("e", "j"), [(i, i + 1) for i in range(ends)])
    below = lax.ppermute(first, ("e", "j"), [(i + 1, i) for i in range(ends)])
    above, below = above.astype(F32), below.astype(F32)
    later = jnp.concatenate([d_conv[1:], below], axis=0)
    earlier = jnp.concatenate([above, d_conv[:-1]], axis=0)
    d_inner = conv_taps[0] * later + conv_taps[1] * d_conv + conv_taps[2] * earlier
    grad_in_gate = (d_inner * conv_input.astype(F32)).astype(BF16)
    grad_conv_input = (d_inner * in_gate.astype(F32)).astype(BF16)
    return (
        grad_resid,
        grad_up,
        grad_down,
        grad_out_gate,
        grad_in_gate,
        grad_conv_input,
        grad_w_out,
    )


def solution(mesh):
    slices, blocks = mesh.shape["sp"], mesh.shape["tp"]
    grid = mesh.devices.reshape(slices // 2, 2, blocks // 2, 2)
    inner = Mesh(grid, ("e", "j", "x", "c"))
    sp, tp = ("e", "j"), ("x", "c")
    in_specs = (
        P(sp, None),
        P(sp, None),
        P(sp, None),
        P(sp, None),
        P(sp, None, tp),
        P(sp, None, tp),
        P(sp, tp, None),
        P(sp, tp),
        P(sp, tp),
        P(sp, tp),
        P(sp, tp),
        P(None, tp),
        P(tp, None),
    )
    out_specs = (
        P(sp, None),
        P(sp, None, tp),
        P(sp, tp, None),
        P(sp, tp),
        P(sp, tp),
        P(sp, tp),
        P(sp, tp),
    )

    return jax.shard_map(
        per_device, mesh=inner, in_specs=in_specs, out_specs=out_specs, check_vma=False
    )
```

```python
import functools

import jax
import jax.numpy as jnp
from jax import lax
from jax.experimental import pallas as pl
from jax.experimental.pallas import tpu as pltpu
from jax.sharding import Mesh
from jax.sharding import PartitionSpec as P


epsilon = 1e-06
F32 = jnp.float32
BF16 = jnp.bfloat16


def swap(value, axis):
    return lax.ppermute(value, axis, [(0, 1), (1, 0)])


def swap_both(value):
    return lax.ppermute(value, ("j", "x"), [(i, 3 - i) for i in range(4)])


def exchange(blocks, sign):
    count = lax.axis_size("e")
    if count <= 8:
        came = []
        for s, b in enumerate(blocks, 1):
            came.append(lax.ppermute(b, "e", [(i, (i + sign * s) % count) for i in range(count)]))
        return came
    mine, order = lax.axis_index("e"), jnp.arange(count)
    to = jnp.take(jnp.stack([blocks[0], *blocks]), sign * (order - mine) % count, axis=0)
    came = lax.all_to_all(to, "e", 0, 0, tiled=True)
    came = jnp.take(came, (mine - sign * order) % count, axis=0)
    return [came[s] for s in range(1, count)]


def dot(a, b, ca, cb):
    return lax.dot_general(a, b, (((ca,), (cb,)), ((), ())), preferred_element_type=F32)


def prepare(experts, cap, quarter, routes_ref, weights_ref, resid_ref, grad_ref, *outs):
    sel_ref = outs[-1]
    sends = ((outs[0], outs[1]), *[(send.at[0], send.at[1]) for send in outs[2:-1]])
    tokens = resid_ref.shape[0]
    mine, column = lax.axis_index("e"), 2 * lax.axis_index("x") + lax.axis_index("c")
    resid = resid_ref[...].astype(F32)
    inv_rms = lax.rsqrt(jnp.mean(resid * resid, axis=-1, keepdims=True) + epsilon)
    cols = pl.ds(pl.multiple_of(column * quarter, quarter), quarter)
    normed = (resid_ref[:, cols].astype(F32) * inv_rms).astype(BF16)
    grad = grad_ref[:, cols]
    first, second = routes_ref[0:1, :], routes_ref[1:2, :]
    first = jnp.where(first >= mine, first - mine, first - mine + experts)
    second = jnp.where(second >= mine, second - mine, second - mine + experts)
    ids = lax.broadcasted_iota(jnp.int32, (experts, tokens), 0)
    in_first, in_second = ids == first, ids == second
    member = jnp.where(in_first | in_second, 1.0, 0.0)
    before = jnp.where(
        lax.broadcasted_iota(jnp.int32, (tokens, tokens), 0)
        < lax.broadcasted_iota(jnp.int32, (tokens, tokens), 1),
        1.0,
        0.0,
    )
    rank = dot(member.astype(BF16), before.astype(BF16), 1, 0)
    rank_first = jnp.sum(jnp.where(in_first, rank, 0.0), axis=0, keepdims=True).astype(jnp.int32)
    rank_second = jnp.sum(jnp.where(in_second, rank, 0.0), axis=0, keepdims=True).astype(jnp.int32)
    slot_first = first * cap + rank_first
    slot_second = second * cap + rank_second
    for step in range(experts):
        slots = lax.broadcasted_iota(jnp.int32, (cap, tokens), 0) + step * cap
        hit_first, hit_second = slots == slot_first, slots == slot_second
        pick = jnp.where(hit_first | hit_second, 1.0, 0.0).astype(BF16)
        share = jnp.where(hit_first, weights_ref[0:1, :], 0.0) + jnp.where(
            hit_second, weights_ref[1:2, :], 0.0
        )
        share = jnp.sum(share, axis=1, keepdims=True)
        sel_ref[step] = pick
        rows_ref, grads_ref = sends[step]
        rows_ref[...] = dot(pick, normed, 1, 0).astype(BF16)
        grads_ref[...] = (share * dot(pick, grad, 1, 0)).astype(BF16)


def columns(place, step, width):
    return pl.ds(pl.multiple_of((place ^ step) * width, width), width)


def activation(rows, gate_ref, up_ref, slope_ref, active_ref, hidden_ref):
    pre_gate = dot(rows, gate_ref[...], 1, 0)
    pre_up = dot(rows, up_ref[...], 1, 0)
    sigmoid_gate = jax.nn.sigmoid(pre_gate)
    activated = pre_gate * sigmoid_gate
    slope_ref[...] = pre_up * sigmoid_gate * (1.0 + pre_gate * (1.0 - sigmoid_gate))
    active_ref[...] = activated
    hidden_ref[...] = (activated * pre_up).astype(BF16)


def first_half(
    cap,
    own_ref,
    own_sib_ref,
    own_y_ref,
    own_y_sib_ref,
    pair_ref,
    pair_sib_ref,
    near_own_ref,
    near_own_sib_ref,
    near_ref,
    near_sib_ref,
    gate_ref,
    up_ref,
    down_ref,
    rows_ref,
    slope_ref,
    active_ref,
    hidden_ref,
    near_out_ref,
    half_ref,
):
    place = 2 * lax.axis_index("x") + lax.axis_index("c")
    quarter = pair_ref.shape[-1]
    count = cap + pair_ref.shape[1]
    sides = (
        (own_ref, own_y_ref, pair_ref, near_own_ref, near_ref),
        (own_sib_ref, own_y_sib_ref, pair_sib_ref, near_own_sib_ref, near_sib_ref),
    )
    for dc, (own, own_y, pair, near_own, near) in enumerate(sides):
        for dx in range(2):
            cols = columns(place, 2 * dx + dc, quarter)
            rows_ref[:cap, cols] = own[dx * cap : (dx + 1) * cap]
            rows_ref[cap:count, cols] = pair[dx]
            rows_ref[count:, cols] = own_y[dx * cap : (dx + 1) * cap]
        cols = slice(dc * quarter, (dc + 1) * quarter)
        for dj in range(2):
            near_out_ref[dj * count : dj * count + cap, cols] = near_own[dj]
            near_out_ref[dj * count + cap : (dj + 1) * count, cols] = near[dj]
    activation(rows_ref[...], gate_ref, up_ref, slope_ref, active_ref, hidden_ref)
    half_ref[...] = dot(
        near_out_ref[:, :quarter], down_ref[:, columns(place, 0, quarter)], 1, 1
    ) + dot(near_out_ref[:, quarter:], down_ref[:, columns(place, 1, quarter)], 1, 1)


def second_half(
    cap,
    rows_y_ref,
    rows_y_sib_ref,
    far_own_ref,
    far_own_sib_ref,
    far_ref,
    far_sib_ref,
    slope_ref,
    active_ref,
    half_ref,
    gate_ref,
    up_ref,
    down_ref,
    rows_ref,
    far_out_ref,
    hidden_ref,
    d_gate_ref,
    d_up_ref,
    away_ref,
    late_slope_ref,
    late_active_ref,
):
    place = 2 * lax.axis_index("x") + lax.axis_index("c")
    quarter = far_ref.shape[-1]
    count = cap + far_ref.shape[1]
    early = slope_ref.shape[0]
    sides = ((rows_y_ref, far_own_ref, far_ref), (rows_y_sib_ref, far_own_sib_ref, far_sib_ref))
    for dc, (rows_y, far_own, far) in enumerate(sides):
        for dx in range(2):
            rows_ref[:, columns(place, 2 * dx + dc, quarter)] = rows_y[dx]
        cols = slice(dc * quarter, (dc + 1) * quarter)
        for dj in range(2):
            far_out_ref[dj * count : dj * count + cap, cols] = far_own[dj]
            far_out_ref[dj * count + cap : (dj + 1) * count, cols] = far[dj]
    activation(rows_ref[...], gate_ref, up_ref, late_slope_ref, late_active_ref, hidden_ref)
    for low, high, slope, active in (
        (0, early, slope_ref, active_ref),
        (early, 2 * count, late_slope_ref, late_active_ref),
    ):
        part = slice(low, high)
        d_hidden = half_ref[part] + (
            dot(far_out_ref[part, :quarter], down_ref[:, columns(place, 2, quarter)], 1, 1)
            + dot(far_out_ref[part, quarter:], down_ref[:, columns(place, 3, quarter)], 1, 1)
        )
        d_gate_ref[part] = (d_hidden * slope[...]).astype(BF16)
        d_up_ref[part] = (d_hidden * active[...]).astype(BF16)
    for dx in range(2):
        block = columns(place, 2 * dx + 1, quarter)
        away_ref[:, dx * quarter : (dx + 1) * quarter] = (
            dot(d_gate_ref[...], gate_ref[block], 1, 1) + dot(d_up_ref[...], up_ref[block], 1, 1)
        ).astype(BF16)


def kept_part(d_gate_ref, d_up_ref, gate_ref, up_ref, kept_ref):
    place = 2 * lax.axis_index("x") + lax.axis_index("c")
    quarter = kept_ref.shape[1] // 2
    for dx in range(2):
        block = columns(place, 2 * dx, quarter)
        kept_ref[:, dx * quarter : (dx + 1) * quarter] = dot(
            d_gate_ref[...], gate_ref[block], 1, 1
        ) + dot(d_up_ref[...], up_ref[block], 1, 1)


def join(kept_ref, other_ref, *block_refs):
    cap, rest, quarter = block_refs[0].shape[0], block_refs[4].shape[0], block_refs[0].shape[1]
    for i in range(4):
        dj, dx = divmod(i, 2)
        cols = slice(dx * quarter, (dx + 1) * quarter)
        start = dj * (cap + rest)
        for block_ref, low, high in (
            (block_refs[i], start, start + cap),
            (block_refs[4 + i], start + cap, start + cap + rest),
        ):
            block_ref[...] = (
                kept_ref[low:high, cols] + other_ref[low:high, cols].astype(F32)
            ).astype(BF16)


def grad_of_down(near_ref, far_ref, early_ref, late_ref, down_ref):
    place = 2 * lax.axis_index("x") + lax.axis_index("c")
    early = early_ref.shape[0]
    quarter = near_ref.shape[1] // 2
    for dx, grads in enumerate((near_ref, far_ref)):
        for dc in range(2):
            cols = slice(dc * quarter, (dc + 1) * quarter)
            down_ref[0, :, columns(place, 2 * dx + dc, quarter)] = (
                dot(early_ref[...], grads[:early, cols], 0, 0)
                + dot(late_ref[...], grads[early:, cols], 0, 0)
            ).astype(BF16)


def grad_of_up(early_ref, late_ref, d_up_ref, up_ref):
    early, features = early_ref.shape
    quarter = features // 4
    for q in range(4):
        cols = slice(q * quarter, (q + 1) * quarter)
        up_ref[0, cols, :] = (
            dot(early_ref[:, cols], d_up_ref[:early], 0, 0)
            + dot(late_ref[:, cols], d_up_ref[early:], 0, 0)
        ).astype(BF16)


def order_mixed(*refs):
    came, outs = refs[:-2], refs[-2:]
    experts = len(came)
    mine, half, core = lax.axis_index("e"), lax.axis_index("j"), lax.axis_index("c")
    _, part, quarter = came[0].shape
    channels = quarter // 2
    for s in range(experts):
        source = jnp.where(mine >= s, mine - s, mine - s + experts)
        for dj in range(2):
            rows = pl.ds(pl.multiple_of((source * 2 + (half ^ dj)) * part, part), part)
            for d in range(2):
                lanes = pl.ds(pl.multiple_of((core ^ d) * channels, channels), channels)
                outs[d][rows] = came[s][dj, :, lanes]


def finish(
    d_normed_ref,
    resid_ref,
    grad_ref,
    w_out_ref,
    conv_ref,
    gate_ref,
    out_ref,
    blocks_ref,
    out_gate_ref,
    d_conv_ref,
    first_ref,
    last_ref,
):
    d_normed = d_normed_ref[...].astype(F32)
    resid = resid_ref[...].astype(F32)
    inv_rms = lax.rsqrt(jnp.mean(resid * resid, axis=-1, keepdims=True) + epsilon)
    unit = resid * inv_rms
    row_mean = jnp.mean(unit * d_normed, axis=-1, keepdims=True)
    grad_resid = (
        grad_ref[...].astype(F32) + inv_rms * (d_normed - unit * row_mean)
    ).astype(BF16)
    out_ref[...] = grad_resid
    count, part, width = blocks_ref.shape
    mine = pl.ds(pl.multiple_of(lax.axis_index("c") * part, part), part)
    for s in range(count):
        blocks_ref[s] = out_ref[mine, s * width : (s + 1) * width]
    d_mix = dot(grad_resid, w_out_ref[...], 1, 1)
    out_gate_ref[...] = (d_mix * conv_ref[...].astype(F32)).astype(BF16)
    d_conv = d_mix * gate_ref[...].astype(F32)
    d_conv_ref[...] = d_conv
    first_ref[...] = d_conv[:1].astype(BF16)
    last_ref[...] = d_conv[-1:].astype(BF16)


def in_vmem(kernel, outs, scratch, flops, limit, *values):
    vmem = pl.BlockSpec(memory_space=pltpu.VMEM)
    return pl.pallas_call(
        kernel,
        out_shape=[jax.ShapeDtypeStruct(shape, kind) for shape, kind in outs],
        in_specs=[vmem] * len(values),
        out_specs=[vmem] * len(outs),
        scratch_shapes=scratch,
        cost_estimate=pl.CostEstimate(flops=flops, bytes_accessed=0, transcendentals=0),
        compiler_params=pltpu.CompilerParams(vmem_limit_bytes=limit),
    )(*values)


def per_device(
    out_grad,
    residual,
    routes,
    route_weights,
    w_gate,
    w_up,
    w_down,
    out_gate,
    in_gate,
    conv_input,
    conv_out,
    conv_taps,
    w_out,
):
    tokens, features = out_grad.shape
    experts = lax.axis_size("e")
    slices = 2 * experts
    cap = -(-(5 * tokens // slices) // 16) * 16
    quarter = features // 4
    outs = in_vmem(
        functools.partial(prepare, experts, cap, quarter),
        [((cap, quarter), BF16)] * 2
        + [((2, cap, quarter), BF16)] * (experts - 1)
        + [((experts, cap, tokens), BF16)],
        [],
        4 * experts * cap * tokens * quarter,
        16 * 2**20,
        *[
            pltpu.with_memory_space_constraint(v, pltpu.HBM)
            for v in (routes.T, route_weights.T, residual, out_grad)
        ],
    )
    own_rows, own_grads, sends, sel = outs[0], outs[1], outs[2:-1], outs[-1]
    conv_f32 = conv_out.astype(F32)
    gate_f32 = out_gate.astype(F32)
    mixed = (gate_f32 * conv_f32).astype(BF16)
    channels = mixed.shape[1]
    part = tokens // 2
    assert 2 * channels == quarter
    mixed_wide = jnp.concatenate([mixed[:part], mixed[part:]], axis=1)

    came = exchange(sends, 1)
    own_rows_x, own_grads_y = lax.optimization_barrier((swap(own_rows, "x"), swap(own_grads, "j")))
    own_pair = jnp.concatenate([own_rows, own_rows_x, mixed_wide], axis=0)
    own_near = jnp.stack([own_grads, own_grads_y])
    own_y = swap(own_pair, "j")
    own_far = swap(own_near, "x")
    came = lax.optimization_barrier(came)
    rows_z = jnp.concatenate([b[0] for b in came], axis=0)
    grads_z = jnp.concatenate([b[1] for b in came], axis=0)
    count = experts * cap

    mixed_mine = jnp.stack([own_pair[2 * cap :], own_y[2 * cap :]])
    mixed_rel = [mixed_mine] + exchange([mixed_mine] * (experts - 1), 1)
    rows_x, grads_y, own_far = lax.optimization_barrier(
        (swap(rows_z, "x"), swap(grads_z, "j"), own_far)
    )
    pair = jnp.stack([rows_z, rows_x])
    near = jnp.stack([grads_z, grads_y])
    own_far_sib = swap(own_far, "c")
    rows_y, far, own_far_sib = lax.optimization_barrier(
        (swap(pair, "j"), swap(near, "x"), own_far_sib)
    )
    weights = (w_gate[0], w_up[0], w_down[0])
    hidden_units = weights[0].shape[1]
    early = count + cap
    grant = 7 * 4 * 2 * count * hidden_units
    sib = lambda value: (value, swap(value, "c"))
    rows_early, slope, active, hidden_early, grads_near, d_half = in_vmem(
        functools.partial(first_half, cap),
        [
            ((early, features), BF16),
            ((early, hidden_units), F32),
            ((early, hidden_units), F32),
            ((early, hidden_units), BF16),
            ((2 * count, features // 2), BF16),
            ((2 * count, hidden_units), F32),
        ],
        [],
        (4 * early + 2 * count) * features * hidden_units,
        grant,
        *sib(own_pair),
        *sib(own_y),
        *sib(pair),
        *sib(own_near),
        *sib(near),
        *weights,
    )
    rows_late, grads_far, hidden_late, d_gate, d_up, away = in_vmem(
        functools.partial(second_half, cap),
        [
            ((2 * count - early, features), BF16),
            ((2 * count, features // 2), BF16),
            ((2 * count - early, hidden_units), BF16),
            ((2 * count, hidden_units), BF16),
            ((2 * count, hidden_units), BF16),
            ((2 * count, features // 2), BF16),
        ],
        [pltpu.VMEM((2 * count - early, hidden_units), F32)] * 2,
        (4 * (2 * count - early) + 6 * count) * features * hidden_units,
        grant,
        *sib(rows_y),
        own_far,
        own_far_sib,
        *sib(far),
        slope,
        active,
        d_half,
        *weights,
    )

    other = swap(away, "c")
    (kept,) = in_vmem(
        kept_part,
        [((2 * count, features // 2), F32)],
        [],
        4 * count * features * hidden_units,
        grant,
        d_gate,
        d_up,
        *weights[:2],
    )
    blocks = in_vmem(
        join,
        [((cap, quarter), BF16)] * 4 + [((count - cap, quarter), BF16)] * 4,
        [],
        2 * count * features,
        grant,
        kept,
        other,
    )

    def spread(parts):
        return [parts[0], swap(parts[1], "x"), swap(parts[2], "j"), swap_both(parts[3])]

    def total(parts):
        return sum(part.astype(F32) for part in parts).astype(BF16)

    own_layer = spread(blocks[:4])
    rest, mixed_rel = lax.optimization_barrier((total(spread(blocks[4:])), mixed_rel))
    back = exchange([rest[s * cap : (s + 1) * cap] for s in range(experts - 1)], -1)
    own_layer, back = lax.optimization_barrier((own_layer, back))
    back = [total(own_layer), *back]

    (grad_down,) = in_vmem(
        grad_of_down,
        [((1, hidden_units, features), BF16)],
        [],
        4 * count * features * hidden_units,
        2 * grant,
        grads_near,
        grads_far,
        hidden_early,
        hidden_late,
    )
    (grad_up,) = in_vmem(
        grad_of_up,
        [((1, features, hidden_units), BF16)],
        [],
        4 * count * features * hidden_units,
        2 * grant,
        rows_early,
        rows_late,
        d_up,
    )

    d_part = dot(
        sel.reshape(experts * cap, tokens), jnp.concatenate(back, axis=0), 0, 0
    ).astype(BF16)
    d_normed = lax.all_gather(d_part, ("x", "c"), axis=1, tiled=True)
    width = features // slices
    cut = slices if width % 128 == 0 else 1
    grad_resid, blocks, grad_out_gate, d_conv, first, last = in_vmem(
        finish,
        [
            ((tokens, features), BF16),
            ((cut, part, features // cut), BF16),
            ((tokens, channels), BF16),
            ((tokens, channels), F32),
            ((1, channels), BF16),
            ((1, channels), BF16),
        ],
        [],
        16 * tokens * features,
        8 * 2**20,
        d_normed,
        residual,
        out_grad,
        w_out,
        conv_out,
        out_gate,
    )

    ordered = in_vmem(
        order_mixed,
        [((slices * part, channels), BF16)] * 2,
        [],
        2 * slices * part * channels,
        grant,
        *mixed_rel,
    )
    if cut == 1:
        blocks = jnp.transpose(blocks.reshape(part, slices, width), (1, 0, 2))
    got = lax.all_to_all(blocks, ("e", "j"), 0, 0, tiled=True).reshape(slices * part, width)
    got_sib = swap(got, "c")
    grad_w_out = dot(got, ordered[0], 0, 0)
    grad_w_out = grad_w_out + dot(got_sib, ordered[1], 0, 0)

    ends = slices - 1
    above = lax.ppermute(last, ("e", "j"), [(i, i + 1) for i in range(ends)])
    below = lax.ppermute(first, ("e", "j"), [(i + 1, i) for i in range(ends)])
    above, below = above.astype(F32), below.astype(F32)
    later = jnp.concatenate([d_conv[1:], below], axis=0)
    earlier = jnp.concatenate([above, d_conv[:-1]], axis=0)
    d_inner = conv_taps[0] * later + conv_taps[1] * d_conv + conv_taps[2] * earlier
    grad_in_gate = (d_inner * conv_input.astype(F32)).astype(BF16)
    grad_conv_input = (d_inner * in_gate.astype(F32)).astype(BF16)
    return (
        grad_resid,
        grad_up,
        grad_down,
        grad_out_gate,
        grad_in_gate,
        grad_conv_input,
        grad_w_out,
    )


def solution(mesh):
    slices, blocks = mesh.shape["sp"], mesh.shape["tp"]
    grid = mesh.devices.reshape(slices // 2, 2, blocks // 2, 2)
    inner = Mesh(grid, ("e", "j", "x", "c"))
    sp, tp = ("e", "j"), ("x", "c")
    in_specs = (
        P(sp, None),
        P(sp, None),
        P(sp, None),
        P(sp, None),
        P(sp, None, tp),
        P(sp, None, tp),
        P(sp, tp, None),
        P(sp, tp),
        P(sp, tp),
        P(sp, tp),
        P(sp, tp),
        P(None, tp),
        P(tp, None),
    )
    out_specs = (
        P(sp, None),
        P(sp, None, tp),
        P(sp, tp, None),
        P(sp, tp),
        P(sp, tp),
        P(sp, tp),
        P(sp, tp),
    )

    return jax.shard_map(
        per_device, mesh=inner, in_specs=in_specs, out_specs=out_specs, check_vma=False
    )
```
